128 devices in a mesh: sp: 64 (over z, y, x), tp: 2 (over core).
Axes of the slice: x: 4, y: 4, z: 4, core: 2. Of those that a mesh axis runs over, the one named last changes fastest.
Arguments:
- stream: bfloat16 [16384, 2048], P(('sp', 'tp')), may hold values from -6 to 6
- outer_gate: bfloat16 [16384, 1024], P('sp', 'tp'), may hold values from -6 to 6
- inner_gate: bfloat16 [16384, 1024], P('sp', 'tp'), may hold values from -6 to 6
- conv_values: bfloat16 [16384, 1024], P('sp', 'tp'), may hold values from -6 to 6
- doc_ids: int32 [16384], P('sp'), may hold values from 0 to 31, never falling along the last dimension, each value on 1 to 1024 neighbouring positions
- conv_taps: float32 [3, 1024], P(None, 'tp'), may hold values from -3.5 to 3.5
- out_weight: bfloat16 [1024, 2048], replicated, may hold values from -0.1875 to 0.1875
- norm_gain: float32 [2048], replicated, may hold values from 0.1 to 1.9
- route_ids: int32 [16384, 2], P(('sp', 'tp')), may hold values from 0 to 127, all different within a row; in each aligned block of 128 rows (0 to 127, 128 to 255, ...) at most 4 rows name the same one
- route_logits: float32 [16384, 2], P(('sp', 'tp')), may hold values from -4 to 4
- group_weight: float32 [16384], P(('sp', 'tp')), may hold values from 0.25 to 1
- w_gate: bfloat16 [128, 2048, 1024], P(('sp', 'tp')), may hold values from -0.125 to 0.125
- w_up: bfloat16 [128, 2048, 1024], P(('sp', 'tp')), may hold values from -0.125 to 0.125
- w_down: bfloat16 [128, 1024, 2048], P(('sp', 'tp')), may hold values from -0.1875 to 0.1875
Outputs:
- result: bfloat16 [16384, 2048], P(('sp', 'tp'))
The draws below stay inside these ranges and needn't reach their ends.
Inputs may be any that keep to these rules, and one draw needn't show every extreme that they name: `route_ids`: the two experts of a token differ. In the rows of one device (aligned blocks of 128 rows) no expert is named more than 4 times, a bound that some block reaches. `doc_ids`: document numbers never fall along the sequence; a document has 1 to 1024 positions and one has exactly 1024.
All inputs are finite; a program needn't handle non-finite values.
Results may differ from the reference program's by a relative error of at most 0.0052.
Values may be sent and summed in bfloat16 or wider, within the bound.
A program may use at most 64 MiB of HBM per device.

```python
import math
import jax
import jax.numpy as jnp
import numpy as np
from jax import lax

D = 2048
CW = 1024
FF = 1024
TOPK = 2
ROWS = 128
TOKENS = 16384
EXPERTS = 128
CAP = 4
DOCS = 32
MOST_DOC = 1024


def levels(key, shape, cuts, least, high):
    def one(axis_at, shards_of):
        steps = jax.random.uniform(jax.random.fold_in(jax.random.fold_in(key, 6), axis_at), (shards_of,), jnp.float32, least / len(cuts), high / len(cuts))
        return jnp.repeat(jnp.exp(steps), shape[axis_at] // shards_of).reshape((-1,) + (1,) * (len(shape) - axis_at - 1))

    level = one(*cuts[0])
    for cut in cuts[1:]:
        level = level * one(*cut)
    return level


def length_profile(number_of, total, limit, lean):
    portions = [(1 << 20) // math.isqrt(grade ** lean) + 1 for grade in range(2, number_of + 1)]
    surplus, given = total - limit - (number_of - 1), [1] * (number_of - 1)
    while surplus > 0:
        movable = [i for i in range(number_of - 1) if given[i] < limit]
        mass, budget = sum([portions[i] for i in movable]), surplus
        for i in movable:
            extra = min(limit - given[i], max(1, budget * portions[i] // mass), surplus)
            given[i] = given[i] + extra
            surplus = surplus - extra
    return np.array([limit] + given)


def ragged(stream_key, count, total, bound, lean):
    if count == 2:
        one = jax.random.randint(stream_key, (), max(1, total - bound), min(bound, total - 1) + 1)
        return jnp.stack([one, total - one])
    tallies = jnp.asarray(length_profile(count, total, bound, lean), jnp.int32)
    twos = (count - 1) // 2
    giver, taker = tallies[1:1 + 2 * twos:2], tallies[2:2 + 2 * twos:2]
    margin = jnp.minimum(giver - 1, bound - taker)
    passed = jax.random.randint(jax.random.fold_in(stream_key, 1), (twos,), 0, 1 << 20) % (margin + 1)
    tallies = tallies.at[1:1 + 2 * twos:2].set(giver - passed).at[2:2 + 2 * twos:2].set(taker + passed)
    return tallies[jax.random.permutation(jax.random.fold_in(stream_key, 2), count)]


def routed_block(rng, own, number, rows, amount, top, bound, slope):
    sequence = jax.random.permutation(rng, amount)
    packed, ordinary = portions_of(amount, rows * top, bound, slope, True), portions_of(amount, rows * top, bound, slope, False)
    places = jnp.arange(amount)

    def named(sizes, turn):
        used = int((sizes > 0).sum())
        fixed = max(1, used // 4)
        passed = fixed + (places - fixed + turn * (used - fixed)) % max(1, amount - fixed)
        return jnp.zeros((amount,), jnp.int32).at[sequence[jnp.where(places < fixed, places, passed)]].set(jnp.asarray(sizes, jnp.int32))

    sizes = jnp.where(number % 4 == 0, named(packed, number // 4), named(ordinary, number - number // 4 - 1))
    mixed = jax.random.permutation(jax.random.fold_in(own, 3), amount)
    donor, taker = mixed[0:amount // 2 * 2:2], mixed[1:amount // 2 * 2:2]
    slack = jnp.minimum(sizes[donor] - 1, bound - sizes[taker]) // 2
    slack = jnp.where((donor == sequence[0]) | (taker == sequence[0]) | (sizes[taker] == 0), 0, jnp.maximum(slack, 0))
    passed = jax.random.randint(jax.random.fold_in(own, 4), (amount // 2,), 0, 1 << 20) % (slack + 1)
    sizes = sizes.at[donor].add(-passed).at[taker].add(passed)
    members = jnp.searchsorted(jnp.cumsum(sizes), jnp.arange(rows * top), side="right").astype(jnp.int32)
    grid = members.reshape(top, rows).T
    grid = grid[jax.random.permutation(jax.random.fold_in(own, 1), rows)]
    turn = jax.random.randint(jax.random.fold_in(own, 2), (rows, 1), 0, top)
    return jnp.take_along_axis(grid, (jnp.arange(top)[None, :] + turn) % top, axis=1)


def portions_of(count, total, bound, lean, full):
    loads = [(1 << 20) // math.isqrt(rank ** lean) + 1 for rank in range(1, count + 1)]
    largest = bound if full else min(bound, max(-(-total // count), total * loads[0] // sum(loads)))
    least = 1 if total - largest >= count - 1 else 0
    counts, surplus = [largest] + [least] * (count - 1), total - largest - least * (count - 1)
    while surplus > 0:
        candidates = [i for i in range(1, count) if counts[i] < largest] or [i for i in range(1, count) if counts[i] < bound]
        mass, remaining = sum([loads[i] for i in candidates]), surplus
        for i in candidates:
            extra = min(bound - counts[i], max(1, remaining * loads[i] // mass), surplus)
            counts[i] = counts[i] + extra
            surplus = surplus - extra
    return np.array(counts)


def noise(stream_key, dims, deviation, bound, pieces=(), held_as=jnp.bfloat16):
    result = jax.random.normal(stream_key, dims, jnp.float32) * deviation
    if len(pieces) > 0:
        result = levels(stream_key, dims, pieces, -0.22, 0.18) * result
    return jnp.clip(result, min=-bound, max=bound).astype(held_as)


def setup_inputs(seed: int = 0) -> dict:
    arg_keys = jax.random.split(jax.random.key(seed), 15)
    stream = noise(arg_keys[0], (TOKENS, D), 1.0, 6.0, ((0, 128),))
    outer_gate = noise(arg_keys[1], (TOKENS, CW), 1.0, 6.0, ((0, 64), (1, 2)))
    inner_gate = noise(arg_keys[2], (TOKENS, CW), 1.0, 6.0, ((0, 64), (1, 2)))
    conv_values = noise(arg_keys[3], (TOKENS, CW), 1.0, 6.0, ((0, 64), (1, 2)))
    doc_ids = jnp.searchsorted(jnp.cumsum(ragged(arg_keys[4], DOCS, TOKENS, MOST_DOC, 1)), jnp.arange(TOKENS), side="right").astype(jnp.int32)
    conv_taps = noise(arg_keys[5], (3, CW), 3 ** -0.5, 3.5, ((1, 2),), jnp.float32)
    out_weight = noise(arg_keys[6], (CW, D), CW ** -0.5, 0.1875)
    norm_gain = jnp.clip(1.0 + 0.18 * jax.random.normal(arg_keys[7], (D,), jnp.float32), 0.1, 1.9)
    route_ids_keys = jax.random.split(jax.random.fold_in(arg_keys[8], 1), TOKENS // ROWS)
    route_ids_turns = jax.random.permutation(jax.random.fold_in(arg_keys[8], 3), TOKENS // ROWS)
    route_ids = jax.vmap(lambda own, number: routed_block(jax.random.fold_in(arg_keys[8], 2), own, number, ROWS, EXPERTS, TOPK, CAP, 2))(route_ids_keys, route_ids_turns).reshape((TOKENS, TOPK))
    route_logits = noise(arg_keys[9], (TOKENS, TOPK), 1.5, 4.0, ((0, 128),), jnp.float32)
    group_weight = jnp.clip(jnp.exp(math.log(1.0) - 1.3862944 * jax.random.uniform(arg_keys[10], (TOKENS,), jnp.float32) ** levels(arg_keys[10], (TOKENS,), ((0, 128),), -0.2, 0.2)), 0.25, 1.0)
    w_gate = noise(arg_keys[11], (EXPERTS, D, FF), D ** -0.5, 0.125, ((0, 128),))
    w_up = noise(arg_keys[12], (EXPERTS, D, FF), D ** -0.5, 0.125, ((0, 128),))
    w_down = noise(arg_keys[13], (EXPERTS, FF, D), FF ** -0.5, 0.1875, ((0, 128),))
    return {"stream": stream, "outer_gate": outer_gate, "inner_gate": inner_gate, "conv_values": conv_values, "doc_ids": doc_ids, "conv_taps": conv_taps, "out_weight": out_weight, "norm_gain": norm_gain, "route_ids": route_ids, "route_logits": route_logits, "group_weight": group_weight, "w_gate": w_gate, "w_up": w_up, "w_down": w_down}


def reference(stream, outer_gate, inner_gate, conv_values, doc_ids, conv_taps, out_weight, norm_gain, route_ids, route_logits, group_weight, w_gate, w_up, w_down):
    product = (inner_gate.astype(jnp.float32) * conv_values.astype(jnp.float32)).astype(jnp.bfloat16)
    prod_f = product.astype(jnp.float32)
    padded = jnp.pad(prod_f, ((1, 1), (0, 0)))
    padded_docs = jnp.pad(doc_ids, (1, 1), constant_values=-1)
    same_prev = (padded_docs[:-2] == doc_ids).astype(jnp.float32)[:, None]
    same_next = (padded_docs[2:] == doc_ids).astype(jnp.float32)[:, None]
    conv = conv_taps[0] * padded[:-2] * same_prev + conv_taps[1] * prod_f + conv_taps[2] * padded[2:] * same_next
    mixed = (outer_gate.astype(jnp.float32) * conv).astype(jnp.bfloat16)
    resid = stream.astype(jnp.float32) + jnp.dot(mixed, out_weight, preferred_element_type=jnp.float32)
    scale = lax.rsqrt(lax.optimization_barrier(jnp.mean(resid * resid, axis=-1, keepdims=True)) + 1e-06)
    normed = (resid * scale * norm_gain).astype(jnp.bfloat16)
    expo = jnp.exp(route_logits)
    gate = group_weight[:, None] * expo / lax.optimization_barrier(jnp.sum(expo, axis=1, keepdims=True))
    flat_ids = route_ids.reshape(-1)
    gate_flat = gate.reshape(-1)
    load = EXPERTS * CAP
    count_all = flat_ids.shape[0]

    def step(total, expert):
        is_hit = flat_ids == expert
        rank = jnp.cumsum(is_hit.astype(jnp.int32)) - 1
        where_to = jnp.where(is_hit, rank, load).astype(jnp.int32)
        pick = jnp.zeros((load,), jnp.int32).at[where_to].set(jnp.arange(count_all, dtype=jnp.int32), mode='drop')
        is_live = jnp.zeros((load,), gate_flat.dtype).at[where_to].set(1.0, mode='drop')
        token_of = pick // TOPK
        rows_in = normed[token_of]
        hidden = (jax.nn.silu(jnp.dot(rows_in, w_gate[expert], preferred_element_type=jnp.float32)) * jnp.dot(rows_in, w_up[expert], preferred_element_type=jnp.float32)).astype(jnp.bfloat16)
        expert_out = jnp.dot(hidden, w_down[expert], preferred_element_type=jnp.float32).astype(jnp.bfloat16)
        weights = gate_flat[pick] * is_live
        total = total.at[token_of].add(expert_out.astype(jnp.float32) * weights[:, None])
        return (total, None)
    total, unused = lax.scan(step, resid, jnp.arange(EXPERTS, dtype=jnp.int32))
    return total.astype(jnp.bfloat16)
```

```python
import functools

import jax
import jax.numpy as jnp
from jax import lax
from jax.experimental import pallas as pl
from jax.experimental.pallas import tpu as pltpu
from jax.sharding import PartitionSpec as P

MESH = pl.DeviceIdType.MESH
STEP = 37
BACK = pow(STEP, -1, 128)
CHUNKS = 4
PER = 32
F32 = jnp.float32
BF = jnp.bfloat16


def padded_2(shard, sides, width):
    for axis, dim in sides:
        size, length = (lax.axis_size(axis), shard.shape[dim])
        up = [(i, (i + 1) % size) for i in range(size - 1)]
        down = [(j, i) for i, j in up]
        last = lax.slice_in_dim(shard, length - width, length, axis=dim)
        leading = lax.slice_in_dim(shard, 0, width, axis=dim)
        before = lax.ppermute(last, axis, up)
        after = lax.ppermute(leading, axis, down)
        shard = jnp.concatenate([before, shard, after], axis=dim)
    return shard


def partner(k, sign, sp, tp):
    o = lax.rem(k * STEP, 128)
    dz, dy, dx, dc = o // 32, lax.rem(o // 8, 4), lax.rem(o // 2, 4), lax.rem(o, 2)
    z, y, x = sp // 16, lax.rem(sp // 4, 4), lax.rem(sp, 4)
    if sign < 0:
        dz, dy, dx = 4 - dz, 4 - dy, 4 - dx
    there = lax.rem(z + dz, 4) * 16 + lax.rem(y + dy, 4) * 4 + lax.rem(x + dx, 4)
    return there, lax.rem(tp + dc, 2)


def dot(a, b):
    return jnp.dot(a, b, preferred_element_type=F32)


def iota(shape, dim):
    return lax.broadcasted_iota(jnp.int32, shape, dim)


def to_row(col, eye):
    return jnp.sum(jnp.where(eye, col, 0.0), axis=0, keepdims=True)


def to_col(row, eye):
    return jnp.sum(jnp.where(eye, row, 0.0), axis=1, keepdims=True)


def kernel(
    normed_ref, resid_ref, ids_ref, logits_ref, gw_ref, wg_hbm, wu_hbm, wd_hbm,
    out_ref,
    wg, wu, wd, nq, fold, unfold, outbox, inbox, outbox2, inbox2, xbuf, hbuf, yq, acc,
    wsem, send1, recv1, send2, recv2,
):
    sp, tp = lax.axis_index("sp"), lax.axis_index("tp")
    loads = [
        pltpu.make_async_copy(wg_hbm.at[0], wg, wsem.at[0]),
        pltpu.make_async_copy(wu_hbm.at[0], wu, wsem.at[1]),
        pltpu.make_async_copy(wd_hbm.at[0], wd, wsem.at[2]),
    ]
    for load in loads:
        load.start()
    barrier = pltpu.get_barrier_semaphore()

    @pl.loop(1, 128)
    def _(k):
        pl.semaphore_signal(barrier, inc=1, device_id=partner(k, 1, sp, tp), device_id_type=MESH)

    eye = iota((128, 128), 0) == iota((128, 128), 1)
    lane = iota((128, 128), 1)
    hot = [(ids_ref[:, k:k + 1] == lane).astype(F32) for k in range(2)]
    before = (iota((128, 128), 0) > lane).astype(BF)
    count = dot(before, (hot[0] + hot[1]).astype(BF))
    z, y, x = sp // 16, lax.rem(sp // 4, 4), lax.rem(sp, 4)
    slots, slot_rows = [], []
    for k in range(2):
        e = ids_ref[:, k:k + 1]
        dz = ((e >> 5) + (4 - z)) & 3
        dy = (((e >> 3) & 3) + (4 - y)) & 3
        dx = (((e >> 1) & 3) + (4 - x)) & 3
        dc = ((e & 1) + (2 - tp)) & 1
        o = dz * 32 + dy * 8 + dx * 2 + dc
        place = (o * BACK) & 127
        rank = jnp.sum(hot[k] * count, axis=1, keepdims=True)
        slot = place.astype(F32) * 4.0 + rank
        slots.append(slot.astype(jnp.int32))
        slot_rows.append(to_row(slot, eye).astype(jnp.int32))
    expo = jnp.exp(logits_ref[...])
    gw = to_col(gw_ref[...], eye)
    total = expo[:, 0:1] + expo[:, 1:2]
    gates = [gw * expo[:, k:k + 1] / total for k in range(2)]

    for q in range(4):
        nq[q * 128:(q + 1) * 128, :] = normed_ref[:, q * 512:(q + 1) * 512]
    m = iota((512, 512), 0)
    n = iota((512, 512), 1)
    fold[...] = (m == (n & 127) * 4 + (n >> 7)).astype(BF)
    unfold[...] = (n == (m & 127) * 4 + (m >> 7)).astype(BF)

    def copy_out(k, c):
        rows = pl.ds(pl.multiple_of(k * 16, 16), 16)
        return pltpu.make_async_remote_copy(
            src_ref=outbox.at[rows], dst_ref=inbox.at[rows], send_sem=send1.at[c], recv_sem=recv1.at[c],
            device_id=partner(k, 1, sp, tp), device_id_type=MESH)

    def copy_back(k, c):
        rows = pl.ds(pl.multiple_of(k * 16, 16), 16)
        return pltpu.make_async_remote_copy(
            src_ref=outbox2.at[rows], dst_ref=inbox2.at[rows], send_sem=send2.at[c], recv_sem=recv2.at[c],
            device_id=partner(k, -1, sp, tp), device_id_type=MESH)

    def pack(c):
        base = c * 512
        at = iota((512, 128), 0) + base
        mine = ((at >> 2) == slot_rows[0]) | ((at >> 2) == slot_rows[1])
        picks = [(mine & ((at & 3) == q)).astype(BF) for q in range(4)]
        packed = dot(jnp.concatenate(picks, axis=1), nq[...])
        outbox[base:base + 512, :] = packed.astype(BF)

    def span(c):
        return pl.ds(16 if c == 0 else c * 512, 496 if c == 0 else 512)

    pack(0)
    pl.semaphore_wait(barrier, 127)
    for c in range(CHUNKS):
        @pl.loop(max(1, c * PER), (c + 1) * PER)
        def _(k):
            copy_out(k, c).start()
        if c + 1 < CHUNKS:
            pack(c + 1)
    inbox[0:16, :] = outbox[0:16, :]
    for load in loads:
        load.wait()

    for c in range(CHUNKS):
        s = span(c)
        pltpu.make_async_copy(inbox.at[s], inbox.at[s], recv1.at[c]).wait()
        for q in range(4):
            xq = dot(unfold[q * 128:(q + 1) * 128, :], inbox[c * 512:(c + 1) * 512, :])
            xbuf[:, q * 512:(q + 1) * 512] = xq.astype(BF)

        @pl.loop(0, 4)
        def _(n):
            cols = pl.ds(pl.multiple_of(n * 256, 256), 256)
            g = dot(xbuf[...], wg[:, cols])
            u = dot(xbuf[...], wu[:, cols])
            hbuf[:, cols] = (g / (1.0 + jnp.exp(-g)) * u).astype(BF)

        @pl.loop(0, 4)
        def _(q):
            cols = pl.ds(pl.multiple_of(q * 512, 512), 512)
            rows = pl.ds(pl.multiple_of(q * 128, 128), 128)
            yq[rows, :] = dot(hbuf[...], wd[:, cols]).astype(BF)

        outbox2[c * 512:(c + 1) * 512, :] = dot(fold[...], yq[...]).astype(BF)

        @pl.loop(max(1, c * PER), (c + 1) * PER)
        def _(k):
            copy_back(k, c).start()
    inbox2[0:16, :] = outbox2[0:16, :]

    for c in range(CHUNKS):
        s = span(c)
        pltpu.make_async_copy(inbox2.at[s], inbox2.at[s], recv2.at[c]).wait()
        at = iota((128, 512), 1) + c * 512
        for q in range(4):
            cols = slice(q * 512, (q + 1) * 512)
            pick = jnp.concatenate([(at == slots[k] * 4 + q).astype(BF) for k in range(2)], axis=0)
            found = dot(pick, inbox2[c * 512:(c + 1) * 512, :])
            if c == 0:
                acc[:, cols] = found
            elif c + 1 < CHUNKS:
                acc[:, cols] += found
            else:
                found = found + acc[:, cols]
                out_ref[:, cols] = (
                    resid_ref[:, cols] + (gates[0] * found[:128] + gates[1] * found[128:])).astype(BF)
    for c in range(CHUNKS):
        s = span(c)
        pltpu.make_async_copy(outbox.at[s], outbox.at[s], send1.at[c]).wait()
        pltpu.make_async_copy(outbox2.at[s], outbox2.at[s], send2.at[c]).wait()


def experts(normed, resid, ids, logits, gw, w_gate, w_up, w_down):
    vmem = pl.BlockSpec(memory_space=pltpu.VMEM)
    hbm = pl.BlockSpec(memory_space=pl.ANY)
    box = pltpu.VMEM((2048, 512), BF)
    sems = pltpu.SemaphoreType.DMA((CHUNKS,))
    return pl.pallas_call(
        kernel,
        out_shape=jax.ShapeDtypeStruct((128, 2048), BF),
        in_specs=[vmem] * 5 + [hbm] * 3,
        out_specs=vmem,
        scratch_shapes=[
            pltpu.VMEM((2048, 1024), BF), pltpu.VMEM((2048, 1024), BF), pltpu.VMEM((1024, 2048), BF),
            pltpu.VMEM((512, 512), BF), pltpu.VMEM((512, 512), BF), pltpu.VMEM((512, 512), BF),
            box, box, box, box,
            pltpu.VMEM((128, 2048), BF), pltpu.VMEM((128, 1024), BF), pltpu.VMEM((512, 512), BF),
            pltpu.VMEM((256, 2048), F32),
            pltpu.SemaphoreType.DMA((3,)), sems, sems, sems, sems,
        ],
        compiler_params=pltpu.CompilerParams(
            collective_id=0, has_side_effects=True, vmem_limit_bytes=50 * 2**20),
        name="experts",
    )(normed, resid, ids, logits, gw, w_gate, w_up, w_down)


def on_device(
    stream, outer_gate, inner_gate, conv_values, doc_ids, conv_taps, out_weight, norm_gain,
    route_ids, route_logits, group_weight, w_gate, w_up, w_down,
):
    product = (inner_gate.astype(F32) * conv_values.astype(F32)).astype(BF)
    doc_float = doc_ids.astype(BF)
    padded, padded_docs = (padded_2(product, (("sp", 0),), 1), padded_2(doc_float, (("sp", 0),), 1))
    same_prev = (padded_docs[:-2] == doc_float).astype(F32)[:, None]
    same_next = (padded_docs[2:] == doc_float).astype(F32)[:, None]
    conv = (
        conv_taps[0] * padded[:-2].astype(F32) * same_prev
        + conv_taps[1] * product.astype(F32)
        + conv_taps[2] * padded[2:].astype(F32) * same_next
    )
    mixed = (outer_gate.astype(F32) * conv).astype(BF)
    channels = lax.all_to_all(mixed, "tp", split_axis=0, concat_axis=1, tiled=True)
    projected = jnp.dot(channels, out_weight, preferred_element_type=F32)
    resid = stream.astype(F32) + projected
    scale = lax.rsqrt(jnp.mean(resid * resid, axis=-1, keepdims=True) + 1e-06)
    normed = (resid * scale * norm_gain).astype(BF)
    return experts(
        normed, resid, route_ids, route_logits, group_weight.reshape(1, 128), w_gate, w_up, w_down)


def solution(mesh):
    placed = (
        P(("sp", "tp"), None),
        P("sp", "tp"),
        P("sp", "tp"),
        P("sp", "tp"),
        P("sp"),
        P(None, "tp"),
        P(),
        P(),
        P(("sp", "tp"), None),
        P(("sp", "tp"), None),
        P(("sp", "tp")),
        P(("sp", "tp"), None, None),
        P(("sp", "tp"), None, None),
        P(("sp", "tp"), None, None),
    )
    return jax.shard_map(
        on_device, mesh=mesh, in_specs=placed, out_specs=P(("sp", "tp"), None), check_vma=False
    )
```

```python
import functools

import jax
import jax.numpy as jnp
from jax import lax
from jax.experimental import pallas as pl
from jax.experimental.pallas import tpu as pltpu
from jax.sharding import PartitionSpec as P

MESH = pl.DeviceIdType.MESH
STEP = 37
BACK = pow(STEP, -1, 128)
CHUNKS = 4
PER = 32
F32 = jnp.float32
BF = jnp.bfloat16


def partner(k, sign, sp, tp):
    o = lax.rem(k * STEP, 128)
    dz, dy, dx, dc = o // 32, lax.rem(o // 8, 4), lax.rem(o // 2, 4), lax.rem(o, 2)
    z, y, x = sp // 16, lax.rem(sp // 4, 4), lax.rem(sp, 4)
    if sign < 0:
        dz, dy, dx = 4 - dz, 4 - dy, 4 - dx
    there = lax.rem(z + dz, 4) * 16 + lax.rem(y + dy, 4) * 4 + lax.rem(x + dx, 4)
    return there, lax.rem(tp + dc, 2)


def dot(a, b):
    return jnp.dot(a, b, preferred_element_type=F32)


def iota(shape, dim):
    return lax.broadcasted_iota(jnp.int32, shape, dim)


def to_row(col, eye):
    return jnp.sum(jnp.where(eye, col, 0.0), axis=0, keepdims=True)


def to_col(row, eye):
    return jnp.sum(jnp.where(eye, row, 0.0), axis=1, keepdims=True)


def kernel(
    stream_hbm, outer_hbm, inner_hbm, values_hbm, docs_hbm, taps_hbm, gain_hbm, ids_hbm, logits_hbm, gw_hbm,
    ow_hbm, wg_hbm, wu_hbm, wd_hbm,
    out_ref,
    inner_ref, values_ref, docs_ref, outer_ref, taps_ref, ids_ref, logits_ref, gw_ref, stream_ref, gain_ref,
    ow, wg, wu, wd, product, mixed, edge_prev, edge_next, docs_prev, docs_next, theirs, resid,
    nq, fold, unfold, outbox, inbox, outbox2, inbox2, xbuf, hbuf, yq, acc,
    wsem, esend, erecv, tsend, trecv, send1, recv1, send2, recv2,
):
    sp, tp = lax.axis_index("sp"), lax.axis_index("tp")
    pairs = [
        (inner_hbm, inner_ref), (values_hbm, values_ref), (docs_hbm, docs_ref), (outer_hbm, outer_ref),
        (taps_hbm, taps_ref), (ids_hbm, ids_ref), (logits_hbm, logits_ref), (gw_hbm, gw_ref),
        (stream_hbm, stream_ref), (gain_hbm, gain_ref), (ow_hbm, ow),
        (wg_hbm.at[0], wg), (wu_hbm.at[0], wu), (wd_hbm.at[0], wd),
    ]
    loads = [pltpu.make_async_copy(a, b, wsem.at[i]) for i, (a, b) in enumerate(pairs)]
    for load in loads:
        load.start()
    barrier = pltpu.get_barrier_semaphore()

    @pl.loop(1, 128)
    def _(k):
        pl.semaphore_signal(barrier, inc=1, device_id=partner(k, 1, sp, tp), device_id_type=MESH)

    for load in loads[:5]:
        load.wait()
    product[...] = (inner_ref[...].astype(F32) * values_ref[...].astype(F32)).astype(BF)
    r0, r1 = iota((256, 256), 0), iota((256, 256), 1)
    docs = docs_ref[...].astype(F32)
    doc = to_col(docs, r0 == r1)
    row = iota((256, 1), 0)
    same_prev = (to_col(docs, r0 == r1 + 1) == doc).astype(F32)
    same_next = (to_col(docs, r0 + 1 == r1) == doc).astype(F32)

    def mix(lo, size, first, last, before, after):
        rows = slice(lo, lo + size)
        own = product[rows, :].astype(F32)
        up, down = pltpu.roll(own, 1, 0), pltpu.roll(own, size - 1, 0)
        at = iota((size, 1), 0)
        if first is not None:
            up = jnp.where(at == 0, first, up)
        if last is not None:
            down = jnp.where(at == size - 1, last, down)
        conv = taps_ref[0:1, :] * up * before + taps_ref[1:2, :] * own + taps_ref[2:3, :] * down * after
        return (outer_ref[rows, :].astype(F32) * conv).astype(BF)

    mixed[...] = mix(0, 256, None, None, same_prev, same_next)

    for load in loads[5:8]:
        load.wait()
    eye = iota((128, 128), 0) == iota((128, 128), 1)
    lane = iota((128, 128), 1)
    ids = [to_col(ids_ref[k:k + 1, :].astype(F32), eye).astype(jnp.int32) for k in range(2)]
    hot = [(ids[k] == lane).astype(F32) for k in range(2)]
    before = (iota((128, 128), 0) > lane).astype(BF)
    count = dot(before, (hot[0] + hot[1]).astype(BF))
    z, y, x = sp // 16, lax.rem(sp // 4, 4), lax.rem(sp, 4)
    slots, slot_rows = [], []
    for k in range(2):
        e = ids[k]
        dz = ((e >> 5) + (4 - z)) & 3
        dy = (((e >> 3) & 3) + (4 - y)) & 3
        dx = (((e >> 1) & 3) + (4 - x)) & 3
        dc = ((e & 1) + (2 - tp)) & 1
        o = dz * 32 + dy * 8 + dx * 2 + dc
        place = (o * BACK) & 127
        rank = jnp.sum(hot[k] * count, axis=1, keepdims=True)
        slot = place.astype(F32) * 4.0 + rank
        slots.append(slot.astype(jnp.int32))
        slot_rows.append(to_row(slot, eye).astype(jnp.int32))
    expo = jnp.exp(logits_ref[...])
    total = expo[0:1, :] + expo[1:2, :]
    gates = [to_col(gw_ref[...] * expo[k:k + 1, :] / total, eye) for k in range(2)]
    m = iota((512, 512), 0)
    n = iota((512, 512), 1)
    fold[...] = (m == (n & 127) * 4 + (n >> 7)).astype(BF)
    unfold[...] = (n == (m & 127) * 4 + (m >> 7)).astype(BF)

    def copy_out(k, c):
        rows = pl.ds(pl.multiple_of(k * 16, 16), 16)
        return pltpu.make_async_remote_copy(
            src_ref=outbox.at[rows], dst_ref=inbox.at[rows], send_sem=send1.at[c], recv_sem=recv1.at[c],
            device_id=partner(k, 1, sp, tp), device_id_type=MESH)

    def copy_back(k, c):
        rows = pl.ds(pl.multiple_of(k * 16, 16), 16)
        return pltpu.make_async_remote_copy(
            src_ref=outbox2.at[rows], dst_ref=inbox2.at[rows], send_sem=send2.at[c], recv_sem=recv2.at[c],
            device_id=partner(k, -1, sp, tp), device_id_type=MESH)

    def pack(c):
        base = c * 512
        at = iota((512, 128), 0) + base
        mine = ((at >> 2) == slot_rows[0]) | ((at >> 2) == slot_rows[1])
        picks = [(mine & ((at & 3) == q)).astype(BF) for q in range(4)]
        packed = dot(jnp.concatenate(picks, axis=1), nq[...])
        outbox[base:base + 512, :] = packed.astype(BF)

    def span(c):
        return pl.ds(16 if c == 0 else c * 512, 496 if c == 0 else 512)

    pl.semaphore_wait(barrier, 127)
    up, down = lax.rem(sp + 1, 64), lax.rem(sp + 63, 64)

    def to_edge(source, target, n, there):
        return pltpu.make_async_remote_copy(
            src_ref=source, dst_ref=target, send_sem=esend.at[n], recv_sem=erecv.at[n],
            device_id=(there, tp), device_id_type=MESH)

    edges = [
        to_edge(product.at[240:256], edge_prev, 0, up),
        to_edge(product.at[0:16], edge_next, 1, down),
        to_edge(docs_ref, docs_prev, 2, up),
        to_edge(docs_ref, docs_next, 3, down),
    ]
    for copy in edges:
        copy.start()

    def to_twin(at, size, n):
        return pltpu.make_async_remote_copy(
            src_ref=mixed.at[pl.ds(pl.multiple_of((1 - tp) * 128 + at, 16), size)],
            dst_ref=theirs.at[pl.ds(pl.multiple_of(at, 16), size)],
            send_sem=tsend.at[n], recv_sem=trecv.at[n], device_id=(sp, 1 - tp), device_id_type=MESH)

    early = to_twin(tp * 16, 112, 0)
    early.start()
    for copy in edges:
        copy.wait()
    zero = (iota((32, 1), 0) == 0) & (sp == 0)
    before = jnp.where(row[:32] == 0, (docs_prev[:, 255:256].astype(F32) == doc[:32]).astype(F32), same_prev[:32])
    before = jnp.where(zero, 0.0, before)
    first = mix(0, 32, edge_prev[15:16, :].astype(F32), None, before, same_next[:32])
    zero = (iota((32, 1), 0) == 31) & (sp == 63)
    after = jnp.where(row[:32] == 31, (docs_next[:, 0:1].astype(F32) == doc[224:]).astype(F32), same_next[224:])
    after = jnp.where(zero, 0.0, after)
    last = mix(224, 32, None, edge_next[0:1, :].astype(F32), same_prev[224:], after)
    mixed[0:16, :] = first[:16]
    mixed[240:256, :] = last[16:]
    late = to_twin((1 - tp) * 112, 16, 1)
    late.start()

    for load in loads[8:11]:
        load.wait()
    mine = pl.ds(pl.multiple_of(tp * 128, 128), 128)
    near = pl.ds(pl.multiple_of(tp * 512, 512), 512)
    far = pl.ds(pl.multiple_of((1 - tp) * 512, 512), 512)
    for q in range(4):
        cols = slice(q * 512, (q + 1) * 512)
        resid[:, cols] = stream_ref[:, cols].astype(F32) + dot(mixed[mine, :], ow[near, cols])
    early.wait()
    late.wait()
    square = jnp.zeros((128, 1), F32)
    for q in range(4):
        cols = slice(q * 512, (q + 1) * 512)
        value = resid[:, cols] + dot(theirs[...], ow[far, cols])
        resid[:, cols] = value
        square += jnp.sum(value * value, axis=1, keepdims=True)
    scale = lax.rsqrt(square / 2048.0 + 1e-06)
    for q in range(4):
        cols = slice(q * 512, (q + 1) * 512)
        nq[q * 128:(q + 1) * 128, :] = (resid[:, cols] * scale * gain_ref[:, cols]).astype(BF)

    pack(0)
    for c in range(CHUNKS):
        @pl.loop(max(1, c * PER), (c + 1) * PER)
        def _(k):
            copy_out(k, c).start()
        if c + 1 < CHUNKS:
            pack(c + 1)
    inbox[0:16, :] = outbox[0:16, :]
    for load in loads[11:]:
        load.wait()

    for c in range(CHUNKS):
        s = span(c)
        pltpu.make_async_copy(inbox.at[s], inbox.at[s], recv1.at[c]).wait()
        for q in range(4):
            xq = dot(unfold[q * 128:(q + 1) * 128, :], inbox[c * 512:(c + 1) * 512, :])
            xbuf[:, q * 512:(q + 1) * 512] = xq.astype(BF)

        @pl.loop(0, 4)
        def _(n):
            cols = pl.ds(pl.multiple_of(n * 256, 256), 256)
            g = dot(xbuf[...], wg[:, cols])
            u = dot(xbuf[...], wu[:, cols])
            hbuf[:, cols] = (g / (1.0 + jnp.exp(-g)) * u).astype(BF)

        @pl.loop(0, 4)
        def _(q):
            cols = pl.ds(pl.multiple_of(q * 512, 512), 512)
            rows = pl.ds(pl.multiple_of(q * 128, 128), 128)
            yq[rows, :] = dot(hbuf[...], wd[:, cols]).astype(BF)

        outbox2[c * 512:(c + 1) * 512, :] = dot(fold[...], yq[...]).astype(BF)

        @pl.loop(max(1, c * PER), (c + 1) * PER)
        def _(k):
            copy_back(k, c).start()
    inbox2[0:16, :] = outbox2[0:16, :]

    for c in range(CHUNKS):
        s = span(c)
        pltpu.make_async_copy(inbox2.at[s], inbox2.at[s], recv2.at[c]).wait()
        at = iota((128, 512), 1) + c * 512
        for q in range(4):
            cols = slice(q * 512, (q + 1) * 512)
            pick = jnp.concatenate([(at == slots[k] * 4 + q).astype(BF) for k in range(2)], axis=0)
            found = dot(pick, inbox2[c * 512:(c + 1) * 512, :])
            if c == 0:
                acc[:, cols] = found
            elif c + 1 < CHUNKS:
                acc[:, cols] += found
            else:
                found = found + acc[:, cols]
                out_ref[:, cols] = (
                    resid[:, cols] + (gates[0] * found[:128] + gates[1] * found[128:])).astype(BF)
    for c in range(CHUNKS):
        s = span(c)
        pltpu.make_async_copy(outbox.at[s], outbox.at[s], send1.at[c]).wait()
        pltpu.make_async_copy(outbox2.at[s], outbox2.at[s], send2.at[c]).wait()


def on_device(
    stream, outer_gate, inner_gate, conv_values, doc_ids, conv_taps, out_weight, norm_gain,
    route_ids, route_logits, group_weight, w_gate, w_up, w_down,
):
    vmem = pl.BlockSpec(memory_space=pltpu.VMEM)
    hbm = pl.BlockSpec(memory_space=pltpu.HBM)
    box = pltpu.VMEM((2048, 512), BF)
    sems = pltpu.SemaphoreType.DMA((CHUNKS,))
    docs = pltpu.VMEM((1, 256), jnp.int32)
    edge = pltpu.VMEM((16, 512), BF)
    return pl.pallas_call(
        kernel,
        out_shape=jax.ShapeDtypeStruct((128, 2048), BF),
        in_specs=[hbm] * 14,
        out_specs=vmem,
        scratch_shapes=[
            pltpu.VMEM((256, 512), BF), pltpu.VMEM((256, 512), BF), docs, pltpu.VMEM((256, 512), BF),
            pltpu.VMEM((3, 512), F32), pltpu.VMEM((2, 128), jnp.int32), pltpu.VMEM((2, 128), F32),
            pltpu.VMEM((1, 128), F32), pltpu.VMEM((128, 2048), BF), pltpu.VMEM((1, 2048), F32),
            pltpu.VMEM((1024, 2048), BF),
            pltpu.VMEM((2048, 1024), BF), pltpu.VMEM((2048, 1024), BF), pltpu.VMEM((1024, 2048), BF),
            pltpu.VMEM((256, 512), BF), pltpu.VMEM((256, 512), BF), edge, edge, docs, docs,
            pltpu.VMEM((128, 512), BF), pltpu.VMEM((128, 2048), F32),
            pltpu.VMEM((512, 512), BF), pltpu.VMEM((512, 512), BF), pltpu.VMEM((512, 512), BF),
            box, box, box, box,
            pltpu.VMEM((128, 2048), BF), pltpu.VMEM((128, 1024), BF), pltpu.VMEM((512, 512), BF),
            pltpu.VMEM((256, 2048), F32),
            pltpu.SemaphoreType.DMA((14,)), pltpu.SemaphoreType.DMA((4,)), pltpu.SemaphoreType.DMA((4,)),
            pltpu.SemaphoreType.DMA((2,)), pltpu.SemaphoreType.DMA((2,)), sems, sems, sems, sems,
        ],
        compiler_params=pltpu.CompilerParams(
            collective_id=0, has_side_effects=True, vmem_limit_bytes=60 * 1024 * 1024),
        name="layer",
    )(
        stream, outer_gate, inner_gate, conv_values, doc_ids.reshape(1, 256), conv_taps,
        norm_gain.reshape(1, 2048), route_ids.T, route_logits.T, group_weight.reshape(1, 128),
        out_weight, w_gate, w_up, w_down)


def solution(mesh):
    placed = (
        P(("sp", "tp"), None),
        P("sp", "tp"),
        P("sp", "tp"),
        P("sp", "tp"),
        P("sp"),
        P(None, "tp"),
        P(),
        P(),
        P(("sp", "tp"), None),
        P(("sp", "tp"), None),
        P(("sp", "tp")),
        P(("sp", "tp"), None, None),
        P(("sp", "tp"), None, None),
        P(("sp", "tp"), None, None),
    )
    return jax.shard_map(
        on_device, mesh=mesh, in_specs=placed, out_specs=P(("sp", "tp"), None), check_vma=False
    )
```

```python
import functools

import jax
import jax.numpy as jnp
from jax import lax
from jax.experimental import pallas as pl
from jax.experimental.pallas import tpu as pltpu
from jax.sharding import PartitionSpec as P

MESH = pl.DeviceIdType.MESH
STEP = 37
BACK = pow(STEP, -1, 128)
CHUNKS = 4
PER = 32
F32 = jnp.float32
BF = jnp.bfloat16


def partner(k, sign, sp, tp):
    o = lax.rem(k * STEP, 128)
    dz, dy, dx, dc = o // 32, lax.rem(o // 8, 4), lax.rem(o // 2, 4), lax.rem(o, 2)
    z, y, x = sp // 16, lax.rem(sp // 4, 4), lax.rem(sp, 4)
    if sign < 0:
        dz, dy, dx = 4 - dz, 4 - dy, 4 - dx
    there = lax.rem(z + dz, 4) * 16 + lax.rem(y + dy, 4) * 4 + lax.rem(x + dx, 4)
    return there, lax.rem(tp + dc, 2)


def dot(a, b):
    return jnp.dot(a, b, preferred_element_type=F32)


def iota(shape, dim):
    return lax.broadcasted_iota(jnp.int32, shape, dim)


def to_row(col, eye):
    return jnp.sum(jnp.where(eye, col, 0.0), axis=0, keepdims=True)


def to_col(row, eye):
    return jnp.sum(jnp.where(eye, row, 0.0), axis=1, keepdims=True)


def kernel(
    stream_hbm, outer_hbm, inner_hbm, values_hbm, docs_hbm, taps_hbm, gain_hbm, ids_hbm, logits_hbm, gw_hbm,
    ow_hbm, wg_hbm, wu_hbm, wd_hbm,
    out_ref,
    inner_ref, values_ref, docs_ref, outer_ref, taps_ref, ids_ref, logits_ref, gw_ref, stream_ref, gain_ref,
    ow, wg, wu, wd, product, mixed, edge, twin_edge, my_edge, docs_near, theirs, resid,
    nq, fold, unfold, outbox, inbox, outbox2, inbox2, xbuf, hbuf, yq, acc,
    wsem, row_sem, plane_sem, esend, erecv, tsend, trecv, send1, recv1, send2, recv2,
):
    sp, tp = lax.axis_index("sp"), lax.axis_index("tp")
    pairs = [
        (inner_hbm, inner_ref), (values_hbm, values_ref), (docs_hbm, docs_ref), (outer_hbm, outer_ref),
        (taps_hbm, taps_ref), (ids_hbm, ids_ref), (logits_hbm, logits_ref), (gw_hbm, gw_ref),
        (stream_hbm, stream_ref), (gain_hbm, gain_ref), (ow_hbm, ow),
        (wg_hbm.at[0], wg), (wu_hbm.at[0], wu), (wd_hbm.at[0], wd),
    ]
    loads = [pltpu.make_async_copy(a, b, wsem.at[i]) for i, (a, b) in enumerate(pairs)]
    for load in loads:
        load.start()
    z, y, x = sp // 16, lax.rem(sp // 4, 4), lax.rem(sp, 4)

    def spot(dz, dy, dx):
        return lax.rem(z + dz, 4) * 16 + lax.rem(y + dy, 4) * 4 + lax.rem(x + dx, 4)

    def signal(sem, there, core):
        pl.semaphore_signal(sem, inc=1, device_id=(there, core), device_id_type=MESH)

    barrier = pltpu.get_barrier_semaphore()
    up, down = lax.rem(sp + 1, 64), lax.rem(sp + 63, 64)
    beside = jnp.where(tp == 0, down, up)
    for core in range(2):
        signal(barrier, beside, core)
    signal(barrier, sp, 1 - tp)
    for d in range(1, 4):
        for core in range(2):
            signal(barrier, spot(0, 0, d), core)
        signal(barrier, spot(0, d, 0), tp)
        signal(barrier, spot(d, 0, 0), tp)

    for load in loads[:3]:
        load.wait()
    product[...] = (inner_ref[...].astype(F32) * values_ref[...].astype(F32)).astype(BF)
    pl.semaphore_wait(barrier, 15)
    for d in range(1, 4):
        signal(row_sem, spot(0, d, 0), tp)

    def to_edge(source, target, n, m, there, core):
        return pltpu.make_async_remote_copy(
            src_ref=source, dst_ref=target, send_sem=esend.at[n], recv_sem=erecv.at[m],
            device_id=(there, core), device_id_type=MESH)

    edges = [
        to_edge(product.at[240:256], edge.at[tp], 0, tp, up, 0),
        to_edge(product.at[0:16], edge.at[tp], 1, tp, down, 1),
        to_edge(docs_ref, docs_near, 2, 2, jnp.where(tp == 0, up, down), tp),
    ]
    for copy in edges:
        copy.start()

    for load in loads[3:5]:
        load.wait()
    r0, r1 = iota((256, 256), 0), iota((256, 256), 1)
    docs = docs_ref[...].astype(F32)
    doc = to_col(docs, r0 == r1)
    same_prev = (to_col(docs, r0 == r1 + 1) == doc).astype(F32)
    same_next = (to_col(docs, r0 + 1 == r1) == doc).astype(F32)
    own = product[...].astype(F32)
    outer = outer_ref[...].astype(F32)
    tap = [taps_ref[k:k + 1, :] for k in range(3)]
    conv = tap[0] * pltpu.roll(own, 1, 0) * same_prev + tap[1] * own + tap[2] * pltpu.roll(own, 255, 0) * same_next
    mixed[...] = (outer * conv).astype(BF)
    base = [
        outer[0:1] * (tap[1] * own[0:1] + tap[2] * own[1:2] * same_next[0:1]),
        outer[255:256] * (tap[1] * own[255:256] + tap[0] * own[254:255] * same_prev[255:256]),
    ]
    coef = [outer[0:1] * tap[0], outer[255:256] * tap[2]]
    here = tp == 0
    my_base, my_coef = jnp.where(here, base[0], base[1]), jnp.where(here, coef[0], coef[1])
    my_edge[...] = jnp.where(
        iota((8, 512), 0) == 0, jnp.where(here, base[1], base[0]), jnp.where(here, coef[1], coef[0]))

    def to_twin(source, target, n):
        return pltpu.make_async_remote_copy(
            src_ref=source, dst_ref=target, send_sem=tsend.at[n], recv_sem=trecv.at[n],
            device_id=(sp, 1 - tp), device_id_type=MESH)

    twins = [
        to_twin(mixed.at[pl.ds(pl.multiple_of((1 - tp) * 128, 128), 128)], theirs, 0),
        to_twin(my_edge, twin_edge, 1),
    ]
    for copy in twins:
        copy.start()
    pl.semaphore_wait(row_sem, 3)
    for d in range(1, 4):
        signal(plane_sem, spot(d, 0, 0), tp)

    for load in loads[5:8]:
        load.wait()
    eye = iota((128, 128), 0) == iota((128, 128), 1)
    lane = iota((128, 128), 1)
    ids = [to_col(ids_ref[k:k + 1, :].astype(F32), eye).astype(jnp.int32) for k in range(2)]
    hot = [(ids[k] == lane).astype(F32) for k in range(2)]
    before = (iota((128, 128), 0) > lane).astype(BF)
    count = dot(before, (hot[0] + hot[1]).astype(BF))
    slots, slot_rows = [], []
    for k in range(2):
        e = ids[k]
        dz = ((e >> 5) + (4 - z)) & 3
        dy = (((e >> 3) & 3) + (4 - y)) & 3
        dx = (((e >> 1) & 3) + (4 - x)) & 3
        dc = ((e & 1) + (2 - tp)) & 1
        o = dz * 32 + dy * 8 + dx * 2 + dc
        place = (o * BACK) & 127
        rank = jnp.sum(hot[k] * count, axis=1, keepdims=True)
        slot = place.astype(F32) * 4.0 + rank
        slots.append(slot.astype(jnp.int32))
        slot_rows.append(to_row(slot, eye).astype(jnp.int32))
    expo = jnp.exp(logits_ref[...])
    total = expo[0:1, :] + expo[1:2, :]
    gates = [to_col(gw_ref[...] * expo[k:k + 1, :] / total, eye) for k in range(2)]
    m = iota((512, 512), 0)
    n = iota((512, 512), 1)
    fold[...] = (m == (n & 127) * 4 + (n >> 7)).astype(BF)
    unfold[...] = (n == (m & 127) * 4 + (m >> 7)).astype(BF)

    def copy_out(k, c):
        rows = pl.ds(pl.multiple_of(k * 16, 16), 16)
        return pltpu.make_async_remote_copy(
            src_ref=outbox.at[rows], dst_ref=inbox.at[rows], send_sem=send1.at[c], recv_sem=recv1.at[c],
            device_id=partner(k, 1, sp, tp), device_id_type=MESH)

    def copy_back(k, c):
        rows = pl.ds(pl.multiple_of(k * 16, 16), 16)
        return pltpu.make_async_remote_copy(
            src_ref=outbox2.at[rows], dst_ref=inbox2.at[rows], send_sem=send2.at[c], recv_sem=recv2.at[c],
            device_id=partner(k, -1, sp, tp), device_id_type=MESH)

    def pack(c):
        base = c * 512
        at = iota((512, 128), 0) + base
        mine = ((at >> 2) == slot_rows[0]) | ((at >> 2) == slot_rows[1])
        picks = [(mine & ((at & 3) == q)).astype(BF) for q in range(4)]
        packed = dot(jnp.concatenate(picks, axis=1), nq[...])
        outbox[base:base + 512, :] = packed.astype(BF)

    def span(c):
        return pl.ds(16 if c == 0 else c * 512, 496 if c == 0 else 512)

    for copy in edges:
        copy.wait_send()
    for half in range(2):
        to_edge(product.at[0:16], edge.at[half], 0, half, up, 0).wait_recv()
    edges[2].wait_recv()
    for copy in twins:
        copy.wait()
    beyond = jnp.where(here, docs_near[:, 255:256], docs_near[:, 0:1])
    at_edge = jnp.where(here, docs_ref[:, 0:1], docs_ref[:, 255:256])
    inside = jnp.where(here, sp > 0, sp < 63)
    same = jnp.where((beyond == at_edge) & inside, 1.0, 0.0)

    def place_edge(box, start, half, base_row, coef_row):
        rows = pl.ds(pl.multiple_of(start + tp * 112, 16), 16)
        block = edge[half].astype(F32)
        near_row = jnp.where(here, block[15:16], block[0:1])
        value = base_row + coef_row * near_row * same
        box[rows, :] = jnp.where(iota((16, 512), 0) == tp * 15, value, box[rows, :].astype(F32)).astype(BF)

    place_edge(mixed, tp * 128, tp, my_base, my_coef)
    place_edge(theirs, 0, 1 - tp, twin_edge[0:1, :], twin_edge[1:2, :])

    for load in loads[8:11]:
        load.wait()
    mine = pl.ds(pl.multiple_of(tp * 128, 128), 128)
    near = pl.ds(pl.multiple_of(tp * 512, 512), 512)
    far = pl.ds(pl.multiple_of((1 - tp) * 512, 512), 512)
    square = jnp.zeros((128, 1), F32)
    for q in range(4):
        cols = slice(q * 512, (q + 1) * 512)
        value = stream_ref[:, cols].astype(F32) + (
            dot(mixed[mine, :], ow[near, cols]) + dot(theirs[...], ow[far, cols]))
        resid[:, cols] = value
        square += jnp.sum(value * value, axis=1, keepdims=True)
    scale = lax.rsqrt(square / 2048.0 + 1e-06)
    for q in range(4):
        cols = slice(q * 512, (q + 1) * 512)
        nq[q * 128:(q + 1) * 128, :] = (resid[:, cols] * scale * gain_ref[:, cols]).astype(BF)

    pack(0)
    pl.semaphore_wait(plane_sem, 3)
    for c in range(CHUNKS):
        @pl.loop(max(1, c * PER), (c + 1) * PER)
        def _(k):
            copy_out(k, c).start()
        if c + 1 < CHUNKS:
            pack(c + 1)
    inbox[0:16, :] = outbox[0:16, :]
    for load in loads[11:]:
        load.wait()

    for c in range(CHUNKS):
        s = span(c)
        pltpu.make_async_copy(inbox.at[s], inbox.at[s], recv1.at[c]).wait()
        for q in range(4):
            xq = dot(unfold[q * 128:(q + 1) * 128, :], inbox[c * 512:(c + 1) * 512, :])
            xbuf[:, q * 512:(q + 1) * 512] = xq.astype(BF)

        @pl.loop(0, 4)
        def _(n):
            cols = pl.ds(pl.multiple_of(n * 256, 256), 256)
            g = dot(xbuf[...], wg[:, cols])
            u = dot(xbuf[...], wu[:, cols])
            hbuf[:, cols] = (g / (1.0 + jnp.exp(-g)) * u).astype(BF)

        @pl.loop(0, 4)
        def _(q):
            cols = pl.ds(pl.multiple_of(q * 512, 512), 512)
            rows = pl.ds(pl.multiple_of(q * 128, 128), 128)
            yq[rows, :] = dot(hbuf[...], wd[:, cols]).astype(BF)

        outbox2[c * 512:(c + 1) * 512, :] = dot(fold[...], yq[...]).astype(BF)

        @pl.loop(max(1, c * PER), (c + 1) * PER)
        def _(k):
            copy_back(k, c).start()
    inbox2[0:16, :] = outbox2[0:16, :]

    for c in range(CHUNKS):
        s = span(c)
        pltpu.make_async_copy(inbox2.at[s], inbox2.at[s], recv2.at[c]).wait()
        at = iota((128, 512), 1) + c * 512
        for q in range(4):
            cols = slice(q * 512, (q + 1) * 512)
            pick = jnp.concatenate([(at == slots[k] * 4 + q).astype(BF) for k in range(2)], axis=0)
            found = dot(pick, inbox2[c * 512:(c + 1) * 512, :])
            if c == 0:
                acc[:, cols] = found
            elif c + 1 < CHUNKS:
                acc[:, cols] += found
            else:
                found = found + acc[:, cols]
                out_ref[:, cols] = (
                    resid[:, cols] + (gates[0] * found[:128] + gates[1] * found[128:])).astype(BF)
    for c in range(CHUNKS):
        s = span(c)
        pltpu.make_async_copy(outbox.at[s], outbox.at[s], send1.at[c]).wait()
        pltpu.make_async_copy(outbox2.at[s], outbox2.at[s], send2.at[c]).wait()


def on_device(
    stream, outer_gate, inner_gate, conv_values, doc_ids, conv_taps, out_weight, norm_gain,
    route_ids, route_logits, group_weight, w_gate, w_up, w_down,
):
    vmem = pl.BlockSpec(memory_space=pltpu.VMEM)
    hbm = pl.BlockSpec(memory_space=pltpu.HBM)
    box = pltpu.VMEM((2048, 512), BF)
    sems = pltpu.SemaphoreType.DMA((CHUNKS,))
    docs = pltpu.VMEM((1, 256), jnp.int32)
    edge = pltpu.VMEM((8, 512), F32)
    return pl.pallas_call(
        kernel,
        out_shape=jax.ShapeDtypeStruct((128, 2048), BF),
        in_specs=[hbm] * 14,
        out_specs=vmem,
        scratch_shapes=[
            pltpu.VMEM((256, 512), BF), pltpu.VMEM((256, 512), BF), docs, pltpu.VMEM((256, 512), BF),
            pltpu.VMEM((3, 512), F32), pltpu.VMEM((2, 128), jnp.int32), pltpu.VMEM((2, 128), F32),
            pltpu.VMEM((1, 128), F32), pltpu.VMEM((128, 2048), BF), pltpu.VMEM((1, 2048), F32),
            pltpu.VMEM((1024, 2048), BF),
            pltpu.VMEM((2048, 1024), BF), pltpu.VMEM((2048, 1024), BF), pltpu.VMEM((1024, 2048), BF),
            pltpu.VMEM((256, 512), BF), pltpu.VMEM((256, 512), BF), pltpu.VMEM((2, 16, 512), BF), edge, edge, docs,
            pltpu.VMEM((128, 512), BF), pltpu.VMEM((128, 2048), F32),
            pltpu.VMEM((512, 512), BF), pltpu.VMEM((512, 512), BF), pltpu.VMEM((512, 512), BF),
            box, box, box, box,
            pltpu.VMEM((128, 2048), BF), pltpu.VMEM((128, 1024), BF), pltpu.VMEM((512, 512), BF),
            pltpu.VMEM((256, 2048), F32),
            pltpu.SemaphoreType.DMA((14,)), pltpu.SemaphoreType.REGULAR, pltpu.SemaphoreType.REGULAR,
            pltpu.SemaphoreType.DMA((3,)), pltpu.SemaphoreType.DMA((3,)),
            pltpu.SemaphoreType.DMA((2,)), pltpu.SemaphoreType.DMA((2,)), sems, sems, sems, sems,
        ],
        compiler_params=pltpu.CompilerParams(
            collective_id=0, has_side_effects=True, vmem_limit_bytes=60 * 1024 * 1024),
        name="layer",
    )(
        stream, outer_gate, inner_gate, conv_values, doc_ids.reshape(1, 256), conv_taps,
        norm_gain.reshape(1, 2048), route_ids.T, route_logits.T, group_weight.reshape(1, 128),
        out_weight, w_gate, w_up, w_down)


def solution(mesh):
    placed = (
        P(("sp", "tp"), None),
        P("sp", "tp"),
        P("sp", "tp"),
        P("sp", "tp"),
        P("sp"),
        P(None, "tp"),
        P(),
        P(),
        P(("sp", "tp"), None),
        P(("sp", "tp"), None),
        P(("sp", "tp")),
        P(("sp", "tp"), None, None),
        P(("sp", "tp"), None, None),
        P(("sp", "tp"), None, None),
    )
    return jax.shard_map(
        on_device, mesh=mesh, in_specs=placed, out_specs=P(("sp", "tp"), None), check_vma=False
    )
```

```python
import functools

import jax
import jax.numpy as jnp
from jax import lax
from jax.experimental import pallas as pl
from jax.experimental.pallas import tpu as pltpu
from jax.sharding import PartitionSpec as P

MESH = pl.DeviceIdType.MESH
STEP = 59
BACK = pow(STEP, -1, 128)
SIZES = (32, 32, 32, 32)
CHUNKS = len(SIZES)
STARTS = [sum(SIZES[:c]) for c in range(CHUNKS)]
F32 = jnp.float32
BF = jnp.bfloat16


def partner(k, sign, sp, tp):
    o = lax.rem(k * STEP, 128)
    dz, dy, dx, dc = o // 32, lax.rem(o // 8, 4), lax.rem(o // 2, 4), lax.rem(o, 2)
    z, y, x = sp // 16, lax.rem(sp // 4, 4), lax.rem(sp, 4)
    if sign < 0:
        dz, dy, dx = 4 - dz, 4 - dy, 4 - dx
    there = lax.rem(z + dz, 4) * 16 + lax.rem(y + dy, 4) * 4 + lax.rem(x + dx, 4)
    return there, lax.rem(tp + dc, 2)


def dot(a, b):
    return jnp.dot(a, b, preferred_element_type=F32)


def iota(shape, dim):
    return lax.broadcasted_iota(jnp.int32, shape, dim)


def to_row(col, eye):
    return jnp.sum(jnp.where(eye, col, 0.0), axis=0, keepdims=True)


def to_col(row, eye):
    return jnp.sum(jnp.where(eye, row, 0.0), axis=1, keepdims=True)


def kernel(
    stream_hbm, outer_hbm, inner_hbm, values_hbm, docs_hbm, taps_hbm, gain_hbm, ids_hbm, logits_hbm, gw_hbm,
    ow_hbm, wg_hbm, wu_hbm, wd_hbm,
    out_ref,
    inner_ref, values_ref, docs_ref, outer_ref, taps_ref, ids_ref, logits_ref, gw_ref, stream_ref, gain_ref,
    ow, wg, wu, wd, product, mixed, edge, twin_edge, my_edge, docs_near, theirs, resid,
    nq, fold, unfold, outbox, inbox, outbox2, inbox2, xbuf, hbuf, yq, acc,
    wsem, row_sem, plane_sem, esend, erecv, tsend, trecv, send1, recv1, send2, recv2,
):
    sp, tp = lax.axis_index("sp"), lax.axis_index("tp")
    pairs = [
        (inner_hbm, inner_ref), (values_hbm, values_ref), (docs_hbm, docs_ref), (outer_hbm, outer_ref),
        (taps_hbm, taps_ref), (ids_hbm, ids_ref), (logits_hbm, logits_ref), (gw_hbm, gw_ref),
        (stream_hbm, stream_ref), (gain_hbm, gain_ref), (ow_hbm, ow),
        (wg_hbm.at[0], wg), (wu_hbm.at[0], wu), (wd_hbm.at[0], wd),
    ]
    loads = [pltpu.make_async_copy(a, b, wsem.at[i]) for i, (a, b) in enumerate(pairs)]
    for load in loads[:11]:
        load.start()
    z, y, x = sp // 16, lax.rem(sp // 4, 4), lax.rem(sp, 4)

    def spot(dz, dy, dx):
        return lax.rem(z + dz, 4) * 16 + lax.rem(y + dy, 4) * 4 + lax.rem(x + dx, 4)

    def signal(sem, there, core):
        pl.semaphore_signal(sem, inc=1, device_id=(there, core), device_id_type=MESH)

    barrier = pltpu.get_barrier_semaphore()
    up, down = lax.rem(sp + 1, 64), lax.rem(sp + 63, 64)
    beside = jnp.where(tp == 0, down, up)
    for core in range(2):
        signal(barrier, beside, core)
    signal(barrier, sp, 1 - tp)
    for d in range(1, 4):
        for core in range(2):
            signal(barrier, spot(0, 0, d), core)
        signal(barrier, spot(0, d, 0), tp)
        signal(barrier, spot(d, 0, 0), tp)

    for load in loads[:3]:
        load.wait()
    product[...] = (inner_ref[...].astype(F32) * values_ref[...].astype(F32)).astype(BF)
    pl.semaphore_wait(barrier, 15)
    for d in range(1, 4):
        signal(row_sem, spot(0, d, 0), tp)

    def to_edge(source, target, n, m, there, core):
        return pltpu.make_async_remote_copy(
            src_ref=source, dst_ref=target, send_sem=esend.at[n], recv_sem=erecv.at[m],
            device_id=(there, core), device_id_type=MESH)

    edges = [
        to_edge(product.at[240:256], edge.at[tp], 0, tp, up, 0),
        to_edge(product.at[0:16], edge.at[tp], 1, tp, down, 1),
        to_edge(docs_ref, docs_near, 2, 2, jnp.where(tp == 0, up, down), tp),
    ]
    for copy in edges:
        copy.start()

    for load in loads[3:5]:
        load.wait()
    r0, r1 = iota((256, 256), 0), iota((256, 256), 1)
    docs = docs_ref[...].astype(F32)
    doc = to_col(docs, r0 == r1)
    same_prev = (to_col(docs, r0 == r1 + 1) == doc).astype(F32)
    same_next = (to_col(docs, r0 + 1 == r1) == doc).astype(F32)
    own = product[...].astype(F32)
    outer = outer_ref[...].astype(F32)
    tap = [taps_ref[k:k + 1, :] for k in range(3)]
    conv = tap[0] * pltpu.roll(own, 1, 0) * same_prev + tap[1] * own + tap[2] * pltpu.roll(own, 255, 0) * same_next
    mixed[...] = (outer * conv).astype(BF)
    base = [
        outer[0:1] * (tap[1] * own[0:1] + tap[2] * own[1:2] * same_next[0:1]),
        outer[255:256] * (tap[1] * own[255:256] + tap[0] * own[254:255] * same_prev[255:256]),
    ]
    coef = [outer[0:1] * tap[0], outer[255:256] * tap[2]]
    here = tp == 0
    my_base, my_coef = jnp.where(here, base[0], base[1]), jnp.where(here, coef[0], coef[1])
    my_edge[...] = jnp.where(
        iota((8, 512), 0) == 0, jnp.where(here, base[1], base[0]), jnp.where(here, coef[1], coef[0]))

    def to_twin(source, target, n):
        return pltpu.make_async_remote_copy(
            src_ref=source, dst_ref=target, send_sem=tsend.at[n], recv_sem=trecv.at[n],
            device_id=(sp, 1 - tp), device_id_type=MESH)

    twins = [
        to_twin(mixed.at[pl.ds(pl.multiple_of((1 - tp) * 128, 128), 128)], theirs, 0),
        to_twin(my_edge, twin_edge, 1),
    ]
    for copy in twins:
        copy.start()
    pl.semaphore_wait(row_sem, 3)
    for d in range(1, 4):
        signal(plane_sem, spot(d, 0, 0), tp)

    for load in loads[5:8]:
        load.wait()
    eye = iota((128, 128), 0) == iota((128, 128), 1)
    lane = iota((128, 128), 1)
    ids = [to_col(ids_ref[k:k + 1, :].astype(F32), eye).astype(jnp.int32) for k in range(2)]
    hot = [(ids[k] == lane).astype(F32) for k in range(2)]
    before = (iota((128, 128), 0) > lane).astype(BF)
    count = dot(before, (hot[0] + hot[1]).astype(BF))
    slots, slot_rows = [], []
    for k in range(2):
        e = ids[k]
        dz = ((e >> 5) + (4 - z)) & 3
        dy = (((e >> 3) & 3) + (4 - y)) & 3
        dx = (((e >> 1) & 3) + (4 - x)) & 3
        dc = ((e & 1) + (2 - tp)) & 1
        o = dz * 32 + dy * 8 + dx * 2 + dc
        place = (o * BACK) & 127
        rank = jnp.sum(hot[k] * count, axis=1, keepdims=True)
        slot = place.astype(F32) * 4.0 + rank
        slots.append(slot.astype(jnp.int32))
        slot_rows.append(to_row(slot, eye).astype(jnp.int32))
    expo = jnp.exp(logits_ref[...])
    total = expo[0:1, :] + expo[1:2, :]
    gates = [to_col(gw_ref[...] * expo[k:k + 1, :] / total, eye) for k in range(2)]

    def copy_out(k, c):
        rows = pl.ds(pl.multiple_of(k * 16, 16), 16)
        return pltpu.make_async_remote_copy(
            src_ref=outbox.at[rows], dst_ref=inbox.at[rows], send_sem=send1.at[c], recv_sem=recv1.at[c],
            device_id=partner(k, 1, sp, tp), device_id_type=MESH)

    def copy_back(k, c):
        rows = pl.ds(pl.multiple_of(k * 16, 16), 16)
        return pltpu.make_async_remote_copy(
            src_ref=outbox2.at[rows], dst_ref=inbox2.at[rows], send_sem=send2.at[c], recv_sem=recv2.at[c],
            device_id=partner(k, -1, sp, tp), device_id_type=MESH)

    def pack(c):
        base, size = STARTS[c] * 16, SIZES[c] * 16
        at = iota((size, 128), 0) + base
        mine = ((at >> 2) == slot_rows[0]) | ((at >> 2) == slot_rows[1])
        picks = [(mine & ((at & 3) == q)).astype(BF) for q in range(4)]
        packed = dot(jnp.concatenate(picks, axis=1), nq[...])
        outbox[base:base + size, :] = packed.astype(BF)

    def span(c):
        first = max(1, STARTS[c])
        return pl.ds(first * 16, (STARTS[c] + SIZES[c] - first) * 16)

    for copy in edges:
        copy.wait_send()
    for half in range(2):
        to_edge(product.at[0:16], edge.at[half], 0, half, up, 0).wait_recv()
    edges[2].wait_recv()
    for copy in twins:
        copy.wait()
    beyond = jnp.where(here, docs_near[:, 255:256], docs_near[:, 0:1])
    at_edge = jnp.where(here, docs_ref[:, 0:1], docs_ref[:, 255:256])
    inside = jnp.where(here, sp > 0, sp < 63)
    same = jnp.where((beyond == at_edge) & inside, 1.0, 0.0)

    def place_edge(box, start, half, base_row, coef_row):
        rows = pl.ds(pl.multiple_of(start + tp * 112, 16), 16)
        block = edge[half].astype(F32)
        near_row = jnp.where(here, block[15:16], block[0:1])
        value = base_row + coef_row * near_row * same
        box[rows, :] = jnp.where(iota((16, 512), 0) == tp * 15, value, box[rows, :].astype(F32)).astype(BF)

    place_edge(mixed, tp * 128, tp, my_base, my_coef)
    place_edge(theirs, 0, 1 - tp, twin_edge[0:1, :], twin_edge[1:2, :])

    for load in loads[8:11]:
        load.wait()
    for load in loads[11:]:
        load.start()
    mine = pl.ds(pl.multiple_of(tp * 128, 128), 128)
    near = pl.ds(pl.multiple_of(tp * 512, 512), 512)
    far = pl.ds(pl.multiple_of((1 - tp) * 512, 512), 512)
    square = jnp.zeros((128, 1), F32)
    for q in range(4):
        cols = slice(q * 512, (q + 1) * 512)
        value = stream_ref[:, cols].astype(F32) + (
            dot(mixed[mine, :], ow[near, cols]) + dot(theirs[...], ow[far, cols]))
        resid[:, cols] = value
        square += jnp.sum(value * value, axis=1, keepdims=True)
    scale = lax.rsqrt(square / 2048.0 + 1e-06)
    for q in range(4):
        cols = slice(q * 512, (q + 1) * 512)
        nq[q * 128:(q + 1) * 128, :] = (resid[:, cols] * scale * gain_ref[:, cols]).astype(BF)

    pack(0)
    pl.semaphore_wait(plane_sem, 3)
    for c in range(CHUNKS):
        @pl.loop(max(1, STARTS[c]), STARTS[c] + SIZES[c])
        def _(k):
            copy_out(k, c).start()
        if c + 1 < CHUNKS:
            pack(c + 1)
    inbox[0:16, :] = outbox[0:16, :]
    m = iota((512, 512), 0)
    n = iota((512, 512), 1)
    fold[...] = (m == (n & 127) * 4 + (n >> 7)).astype(BF)
    unfold[...] = (n == (m & 127) * 4 + (m >> 7)).astype(BF)
    for load in loads[11:]:
        load.wait()

    for c in range(CHUNKS):
        s = span(c)
        pltpu.make_async_copy(inbox.at[s], inbox.at[s], recv1.at[c]).wait()
        box = slice(STARTS[c] * 16, (STARTS[c] + SIZES[c]) * 16)
        rows, size = SIZES[c] * 4, SIZES[c] * 16
        for q in range(4):
            xq = dot(unfold[q * 128:q * 128 + rows, :size], inbox[box, :])
            xbuf[:rows, q * 512:(q + 1) * 512] = xq.astype(BF)

        @pl.loop(0, 4)
        def _(n):
            cols = pl.ds(pl.multiple_of(n * 256, 256), 256)
            g = dot(xbuf[:rows, :], wg[:, cols])
            u = dot(xbuf[:rows, :], wu[:, cols])
            hbuf[:rows, cols] = (g / (1.0 + jnp.exp(-g)) * u).astype(BF)

        @pl.loop(0, 4)
        def _(q):
            cols = pl.ds(pl.multiple_of(q * 512, 512), 512)
            yq[pl.ds(pl.multiple_of(q * 128, 128), rows), :] = dot(hbuf[:rows, :], wd[:, cols]).astype(BF)

        outbox2[box, :] = dot(fold[:size, :], yq[...]).astype(BF)

        @pl.loop(max(1, STARTS[c]), STARTS[c] + SIZES[c])
        def _(k):
            copy_back(k, c).start()
    inbox2[0:16, :] = outbox2[0:16, :]

    for c in range(CHUNKS):
        s = span(c)
        pltpu.make_async_copy(inbox2.at[s], inbox2.at[s], recv2.at[c]).wait()
        box = slice(STARTS[c] * 16, (STARTS[c] + SIZES[c]) * 16)
        at = iota((128, SIZES[c] * 16), 1) + STARTS[c] * 16
        for q in range(4):
            cols = slice(q * 512, (q + 1) * 512)
            pick = jnp.concatenate([(at == slots[k] * 4 + q).astype(BF) for k in range(2)], axis=0)
            found = dot(pick, inbox2[box, :])
            if c == 0:
                acc[:, cols] = found
            elif c + 1 < CHUNKS:
                acc[:, cols] += found
            else:
                found = found + acc[:, cols]
                out_ref[:, cols] = (
                    resid[:, cols] + (gates[0] * found[:128] + gates[1] * found[128:])).astype(BF)
    for c in range(CHUNKS):
        s = span(c)
        pltpu.make_async_copy(outbox.at[s], outbox.at[s], send1.at[c]).wait()
        pltpu.make_async_copy(outbox2.at[s], outbox2.at[s], send2.at[c]).wait()


def on_device(
    stream, outer_gate, inner_gate, conv_values, doc_ids, conv_taps, out_weight, norm_gain,
    route_ids, route_logits, group_weight, w_gate, w_up, w_down,
):
    vmem = pl.BlockSpec(memory_space=pltpu.VMEM)
    hbm = pl.BlockSpec(memory_space=pltpu.HBM)
    box = pltpu.VMEM((2048, 512), BF)
    sems = pltpu.SemaphoreType.DMA((CHUNKS,))
    docs = pltpu.VMEM((1, 256), jnp.int32)
    edge = pltpu.VMEM((8, 512), F32)
    return pl.pallas_call(
        kernel,
        out_shape=jax.ShapeDtypeStruct((128, 2048), BF),
        in_specs=[hbm] * 14,
        out_specs=vmem,
        scratch_shapes=[
            pltpu.VMEM((256, 512), BF), pltpu.VMEM((256, 512), BF), docs, pltpu.VMEM((256, 512), BF),
            pltpu.VMEM((3, 512), F32), pltpu.VMEM((2, 128), jnp.int32), pltpu.VMEM((2, 128), F32),
            pltpu.VMEM((1, 128), F32), pltpu.VMEM((128, 2048), BF), pltpu.VMEM((1, 2048), F32),
            pltpu.VMEM((1024, 2048), BF),
            pltpu.VMEM((2048, 1024), BF), pltpu.VMEM((2048, 1024), BF), pltpu.VMEM((1024, 2048), BF),
            pltpu.VMEM((256, 512), BF), pltpu.VMEM((256, 512), BF), pltpu.VMEM((2, 16, 512), BF), edge, edge, docs,
            pltpu.VMEM((128, 512), BF), pltpu.VMEM((128, 2048), F32),
            pltpu.VMEM((512, 512), BF), pltpu.VMEM((512, 512), BF), pltpu.VMEM((512, 512), BF),
            box, box, box, box,
            pltpu.VMEM((128, 2048), BF), pltpu.VMEM((128, 1024), BF), pltpu.VMEM((512, 512), BF),
            pltpu.VMEM((256, 2048), F32),
            pltpu.SemaphoreType.DMA((14,)), pltpu.SemaphoreType.REGULAR, pltpu.SemaphoreType.REGULAR,
            pltpu.SemaphoreType.DMA((3,)), pltpu.SemaphoreType.DMA((3,)),
            pltpu.SemaphoreType.DMA((2,)), pltpu.SemaphoreType.DMA((2,)), sems, sems, sems, sems,
        ],
        compiler_params=pltpu.CompilerParams(
            collective_id=0, has_side_effects=True, vmem_limit_bytes=44 * 2**20),
        name="layer",
    )(*[pltpu.with_memory_space_constraint(a, pltpu.HBM) for a in (
        stream, outer_gate, inner_gate, conv_values, doc_ids.reshape(1, 256), conv_taps,
        norm_gain.reshape(1, 2048), route_ids.T, route_logits.T, group_weight.reshape(1, 128),
        out_weight, w_gate, w_up, w_down)])


def solution(mesh):
    placed = (
        P(("sp", "tp"), None),
        P("sp", "tp"),
        P("sp", "tp"),
        P("sp", "tp"),
        P("sp"),
        P(None, "tp"),
        P(),
        P(),
        P(("sp", "tp"), None),
        P(("sp", "tp"), None),
        P(("sp", "tp")),
        P(("sp", "tp"), None, None),
        P(("sp", "tp"), None, None),
        P(("sp", "tp"), None, None),
    )
    return jax.shard_map(
        on_device, mesh=mesh, in_specs=placed, out_specs=P(("sp", "tp"), None), check_vma=False
    )
```

```python
import functools

import jax
import jax.numpy as jnp
from jax import lax
from jax.experimental import pallas as pl
from jax.experimental.pallas import tpu as pltpu
from jax.sharding import PartitionSpec as P

MESH = pl.DeviceIdType.MESH
STEP = 59
BACK = pow(STEP, -1, 128)
SIZES = (32, 32, 32, 32)
CHUNKS = len(SIZES)
STARTS = [sum(SIZES[:c]) for c in range(CHUNKS)]
F32 = jnp.float32
BF = jnp.bfloat16


def partner(k, sign, sp, tp):
    o = lax.rem(k * STEP, 128)
    dz, dy, dx, dc = o // 32, lax.rem(o // 8, 4), lax.rem(o // 2, 4), lax.rem(o, 2)
    z, y, x = sp // 16, lax.rem(sp // 4, 4), lax.rem(sp, 4)
    if sign < 0:
        dz, dy, dx = 4 - dz, 4 - dy, 4 - dx
    there = lax.rem(z + dz, 4) * 16 + lax.rem(y + dy, 4) * 4 + lax.rem(x + dx, 4)
    return there, lax.rem(tp + dc, 2)


def dot(a, b):
    return jnp.dot(a, b, preferred_element_type=F32)


def iota(shape, dim):
    return lax.broadcasted_iota(jnp.int32, shape, dim)


def to_row(col, eye):
    return jnp.sum(jnp.where(eye, col, 0.0), axis=0, keepdims=True)


def to_col(row, eye):
    return jnp.sum(jnp.where(eye, row, 0.0), axis=1, keepdims=True)


def kernel(
    stream_hbm, outer_hbm, inner_hbm, values_hbm, docs_hbm, taps_hbm, gain_hbm, ids_hbm, logits_hbm, gw_hbm,
    ow_hbm, wg_hbm, wu_hbm, wd_hbm,
    out_ref,
    inner_ref, values_ref, docs_ref, outer_ref, taps_ref, ids_ref, logits_ref, gw_ref, stream_ref, gain_ref,
    ow, wg, wu, wd, product, mixed, edge, twin_edge, my_edge, docs_near, theirs, resid,
    nq, fold, unfold, outbox, inbox, outbox2, inbox2, xbuf, hbuf, yq, acc, masks,
    wsem, row_sem, plane_sem, esend, erecv, tsend, trecv, send1, recv1, send2, recv2,
):
    sp, tp = lax.axis_index("sp"), lax.axis_index("tp")
    pairs = [
        (inner_hbm, inner_ref), (values_hbm, values_ref), (docs_hbm, docs_ref), (outer_hbm, outer_ref),
        (taps_hbm, taps_ref), (ids_hbm, ids_ref), (logits_hbm, logits_ref), (gw_hbm, gw_ref),
        (stream_hbm, stream_ref), (gain_hbm, gain_ref), (ow_hbm, ow),
        (wg_hbm.at[0], wg), (wu_hbm.at[0], wu), (wd_hbm.at[0], wd),
    ]
    loads = [pltpu.make_async_copy(a, b, wsem.at[i]) for i, (a, b) in enumerate(pairs)]
    for load in loads[:11]:
        load.start()
    z, y, x = sp // 16, lax.rem(sp // 4, 4), lax.rem(sp, 4)

    def spot(dz, dy, dx):
        return lax.rem(z + dz, 4) * 16 + lax.rem(y + dy, 4) * 4 + lax.rem(x + dx, 4)

    def signal(sem, there, core):
        pl.semaphore_signal(sem, inc=1, device_id=(there, core), device_id_type=MESH)

    barrier = pltpu.get_barrier_semaphore()
    up, down = lax.rem(sp + 1, 64), lax.rem(sp + 63, 64)
    beside = jnp.where(tp == 0, down, up)
    for core in range(2):
        signal(barrier, beside, core)
    signal(barrier, sp, 1 - tp)
    for d in range(1, 4):
        for core in range(2):
            signal(barrier, spot(0, 0, d), core)
        signal(barrier, spot(0, d, 0), tp)
        signal(barrier, spot(d, 0, 0), tp)

    for load in loads[:3]:
        load.wait()
    product[...] = (inner_ref[...].astype(F32) * values_ref[...].astype(F32)).astype(BF)
    pl.semaphore_wait(barrier, 15)
    for d in range(1, 4):
        signal(row_sem, spot(0, d, 0), tp)

    def to_edge(source, target, n, m, there, core):
        return pltpu.make_async_remote_copy(
            src_ref=source, dst_ref=target, send_sem=esend.at[n], recv_sem=erecv.at[m],
            device_id=(there, core), device_id_type=MESH)

    edges = [
        to_edge(product.at[240:256], edge.at[tp], 0, tp, up, 0),
        to_edge(product.at[0:16], edge.at[tp], 1, tp, down, 1),
        to_edge(docs_ref, docs_near, 2, 2, jnp.where(tp == 0, up, down), tp),
    ]
    for copy in edges:
        copy.start()

    for load in loads[3:5]:
        load.wait()
    r0, r1 = iota((256, 256), 0), iota((256, 256), 1)
    docs = docs_ref[...].astype(F32)
    doc = to_col(docs, r0 == r1)
    same_prev = (to_col(docs, r0 == r1 + 1) == doc).astype(F32)
    same_next = (to_col(docs, r0 + 1 == r1) == doc).astype(F32)
    own = product[...].astype(F32)
    outer = outer_ref[...].astype(F32)
    tap = [taps_ref[k:k + 1, :] for k in range(3)]
    conv = tap[0] * pltpu.roll(own, 1, 0) * same_prev + tap[1] * own + tap[2] * pltpu.roll(own, 255, 0) * same_next
    mixed[...] = (outer * conv).astype(BF)
    base = [
        outer[0:1] * (tap[1] * own[0:1] + tap[2] * own[1:2] * same_next[0:1]),
        outer[255:256] * (tap[1] * own[255:256] + tap[0] * own[254:255] * same_prev[255:256]),
    ]
    coef = [outer[0:1] * tap[0], outer[255:256] * tap[2]]
    here = tp == 0
    my_base, my_coef = jnp.where(here, base[0], base[1]), jnp.where(here, coef[0], coef[1])
    my_edge[...] = jnp.where(
        iota((8, 512), 0) == 0, jnp.where(here, base[1], base[0]), jnp.where(here, coef[1], coef[0]))

    def to_twin(source, target, n):
        return pltpu.make_async_remote_copy(
            src_ref=source, dst_ref=target, send_sem=tsend.at[n], recv_sem=trecv.at[n],
            device_id=(sp, 1 - tp), device_id_type=MESH)

    twins = [
        to_twin(mixed.at[pl.ds(pl.multiple_of((1 - tp) * 128, 128), 128)], theirs, 0),
        to_twin(my_edge, twin_edge, 1),
    ]
    for copy in twins:
        copy.start()
    pl.semaphore_wait(row_sem, 3)
    for d in range(1, 4):
        signal(plane_sem, spot(d, 0, 0), tp)

    for load in loads[5:8]:
        load.wait()
    eye = iota((128, 128), 0) == iota((128, 128), 1)
    lane = iota((128, 128), 1)
    ids = [to_col(ids_ref[k:k + 1, :].astype(F32), eye).astype(jnp.int32) for k in range(2)]
    hot = [(ids[k] == lane).astype(F32) for k in range(2)]
    before = (iota((128, 128), 0) > lane).astype(BF)
    count = dot(before, (hot[0] + hot[1]).astype(BF))
    slots, slot_rows = [], []
    for k in range(2):
        e = ids[k]
        dz = ((e >> 5) + (4 - z)) & 3
        dy = (((e >> 3) & 3) + (4 - y)) & 3
        dx = (((e >> 1) & 3) + (4 - x)) & 3
        dc = ((e & 1) + (2 - tp)) & 1
        o = dz * 32 + dy * 8 + dx * 2 + dc
        place = (o * BACK) & 127
        rank = jnp.sum(hot[k] * count, axis=1, keepdims=True)
        slot = place.astype(F32) * 4.0 + rank
        slots.append(slot.astype(jnp.int32))
        slot_rows.append(to_row(slot, eye).astype(jnp.int32))
    expo = jnp.exp(logits_ref[...])
    total = expo[0:1, :] + expo[1:2, :]
    gates = [to_col(gw_ref[...] * expo[k:k + 1, :] / total, eye) for k in range(2)]

    def copy_out(k, c):
        rows = pl.ds(pl.multiple_of(k * 16, 16), 16)
        return pltpu.make_async_remote_copy(
            src_ref=outbox.at[rows], dst_ref=inbox.at[rows], send_sem=send1.at[c], recv_sem=recv1.at[c],
            device_id=partner(k, 1, sp, tp), device_id_type=MESH)

    def copy_back(k, c):
        rows = pl.ds(pl.multiple_of(k * 16, 16), 16)
        return pltpu.make_async_remote_copy(
            src_ref=outbox2.at[rows], dst_ref=inbox2.at[rows], send_sem=send2.at[c], recv_sem=recv2.at[c],
            device_id=partner(k, -1, sp, tp), device_id_type=MESH)

    def mask(c):
        base, size = STARTS[c] * 16, SIZES[c] * 16
        at = iota((size, 128), 0) + base
        mine = ((at >> 2) == slot_rows[0]) | ((at >> 2) == slot_rows[1])
        return jnp.concatenate([(mine & ((at & 3) == q)).astype(BF) for q in range(4)], axis=1)

    def pack(c, chosen):
        base, size = STARTS[c] * 16, SIZES[c] * 16
        outbox[base:base + size, :] = dot(chosen, nq[...]).astype(BF)

    def picks(c, q):
        at = iota((128, SIZES[c] * 16), 1) + STARTS[c] * 16
        return jnp.concatenate([(at == slots[k] * 4 + q).astype(BF) for k in range(2)], axis=0)

    def span(c):
        first = max(1, STARTS[c])
        return pl.ds(first * 16, (STARTS[c] + SIZES[c] - first) * 16)

    masks[:512, :] = mask(0)
    for copy in edges:
        copy.wait_send()
    for half in range(2):
        to_edge(product.at[0:16], edge.at[half], 0, half, up, 0).wait_recv()
    edges[2].wait_recv()
    for copy in twins:
        copy.wait()
    beyond = jnp.where(here, docs_near[:, 255:256], docs_near[:, 0:1])
    at_edge = jnp.where(here, docs_ref[:, 0:1], docs_ref[:, 255:256])
    inside = jnp.where(here, sp > 0, sp < 63)
    same = jnp.where((beyond == at_edge) & inside, 1.0, 0.0)

    def place_edge(box, start, half, base_row, coef_row):
        rows = pl.ds(pl.multiple_of(start + tp * 112, 16), 16)
        block = edge[half].astype(F32)
        near_row = jnp.where(here, block[15:16], block[0:1])
        value = base_row + coef_row * near_row * same
        box[rows, :] = jnp.where(iota((16, 512), 0) == tp * 15, value, box[rows, :].astype(F32)).astype(BF)

    place_edge(mixed, tp * 128, tp, my_base, my_coef)
    place_edge(theirs, 0, 1 - tp, twin_edge[0:1, :], twin_edge[1:2, :])

    for load in loads[8:11]:
        load.wait()
    for load in loads[11:]:
        load.start()
    mine = pl.ds(pl.multiple_of(tp * 128, 128), 128)
    near = pl.ds(pl.multiple_of(tp * 512, 512), 512)
    far = pl.ds(pl.multiple_of((1 - tp) * 512, 512), 512)
    square = jnp.zeros((128, 1), F32)
    for q in range(4):
        cols = slice(q * 512, (q + 1) * 512)
        value = stream_ref[:, cols].astype(F32) + (
            dot(mixed[mine, :], ow[near, cols]) + dot(theirs[...], ow[far, cols]))
        resid[:, cols] = value
        square += jnp.sum(value * value, axis=1, keepdims=True)
    scale = lax.rsqrt(square / 2048.0 + 1e-06)
    for q in range(4):
        cols = slice(q * 512, (q + 1) * 512)
        nq[q * 128:(q + 1) * 128, :] = (resid[:, cols] * scale * gain_ref[:, cols]).astype(BF)

    pack(0, masks[:512, :])
    pl.semaphore_wait(plane_sem, 3)
    for c in range(CHUNKS):
        @pl.loop(max(1, STARTS[c]), STARTS[c] + SIZES[c])
        def _(k):
            copy_out(k, c).start()
        if c + 1 < CHUNKS:
            pack(c + 1, mask(c + 1))
    inbox[0:16, :] = outbox[0:16, :]
    m = iota((512, 512), 0)
    n = iota((512, 512), 1)
    fold[...] = (m == (n & 127) * 4 + (n >> 7)).astype(BF)
    unfold[...] = (n == (m & 127) * 4 + (m >> 7)).astype(BF)
    for load in loads[11:]:
        load.wait()

    for c in range(CHUNKS):
        s = span(c)
        pltpu.make_async_copy(inbox.at[s], inbox.at[s], recv1.at[c]).wait()
        box = slice(STARTS[c] * 16, (STARTS[c] + SIZES[c]) * 16)
        rows, size = SIZES[c] * 4, SIZES[c] * 16
        for q in range(4):
            xq = dot(unfold[q * 128:q * 128 + rows, :size], inbox[box, :])
            xbuf[:rows, q * 512:(q + 1) * 512] = xq.astype(BF)

        @pl.loop(0, 4)
        def _(n):
            cols = pl.ds(pl.multiple_of(n * 256, 256), 256)
            g = dot(xbuf[:rows, :], wg[:, cols])
            u = dot(xbuf[:rows, :], wu[:, cols])
            hbuf[:rows, cols] = (g / (1.0 + jnp.exp(-g)) * u).astype(BF)

        @pl.loop(0, 4)
        def _(q):
            cols = pl.ds(pl.multiple_of(q * 512, 512), 512)
            yq[pl.ds(pl.multiple_of(q * 128, 128), rows), :] = dot(hbuf[:rows, :], wd[:, cols]).astype(BF)

        outbox2[box, :] = dot(fold[:size, :], yq[...]).astype(BF)

        @pl.loop(max(1, STARTS[c]), STARTS[c] + SIZES[c])
        def _(k):
            copy_back(k, c).start()
    inbox2[0:16, :] = outbox2[0:16, :]

    for c in range(CHUNKS):
        s = span(c)
        final = c + 1 == CHUNKS
        if final:
            for q in range(4):
                masks[q * 256:(q + 1) * 256, :] = picks(c, q)
        pltpu.make_async_copy(inbox2.at[s], inbox2.at[s], recv2.at[c]).wait()
        box = slice(STARTS[c] * 16, (STARTS[c] + SIZES[c]) * 16)
        for q in range(4):
            cols = slice(q * 512, (q + 1) * 512)
            pick = masks[q * 256:(q + 1) * 256, :] if final else picks(c, q)
            found = dot(pick, inbox2[box, :])
            if c == 0:
                acc[:, cols] = found
            elif c + 1 < CHUNKS:
                acc[:, cols] += found
            else:
                found = found + acc[:, cols]
                out_ref[:, cols] = (
                    resid[:, cols] + (gates[0] * found[:128] + gates[1] * found[128:])).astype(BF)
    for c in range(CHUNKS):
        s = span(c)
        pltpu.make_async_copy(outbox.at[s], outbox.at[s], send1.at[c]).wait()
        pltpu.make_async_copy(outbox2.at[s], outbox2.at[s], send2.at[c]).wait()


def on_device(
    stream, outer_gate, inner_gate, conv_values, doc_ids, conv_taps, out_weight, norm_gain,
    route_ids, route_logits, group_weight, w_gate, w_up, w_down,
):
    vmem = pl.BlockSpec(memory_space=pltpu.VMEM)
    hbm = pl.BlockSpec(memory_space=pltpu.HBM)
    box = pltpu.VMEM((2048, 512), BF)
    sems = pltpu.SemaphoreType.DMA((CHUNKS,))
    docs = pltpu.VMEM((1, 256), jnp.int32)
    edge = pltpu.VMEM((8, 512), F32)
    return pl.pallas_call(
        kernel,
        out_shape=jax.ShapeDtypeStruct((128, 2048), BF),
        in_specs=[hbm] * 14,
        out_specs=vmem,
        scratch_shapes=[
            pltpu.VMEM((256, 512), BF), pltpu.VMEM((256, 512), BF), docs, pltpu.VMEM((256, 512), BF),
            pltpu.VMEM((3, 512), F32), pltpu.VMEM((2, 128), jnp.int32), pltpu.VMEM((2, 128), F32),
            pltpu.VMEM((1, 128), F32), pltpu.VMEM((128, 2048), BF), pltpu.VMEM((1, 2048), F32),
            pltpu.VMEM((1024, 2048), BF),
            pltpu.VMEM((2048, 1024), BF), pltpu.VMEM((2048, 1024), BF), pltpu.VMEM((1024, 2048), BF),
            pltpu.VMEM((256, 512), BF), pltpu.VMEM((256, 512), BF), pltpu.VMEM((2, 16, 512), BF), edge, edge, docs,
            pltpu.VMEM((128, 512), BF), pltpu.VMEM((128, 2048), F32),
            pltpu.VMEM((512, 512), BF), pltpu.VMEM((512, 512), BF), pltpu.VMEM((512, 512), BF),
            box, box, box, box,
            pltpu.VMEM((128, 2048), BF), pltpu.VMEM((128, 1024), BF), pltpu.VMEM((512, 512), BF),
            pltpu.VMEM((256, 2048), F32), pltpu.VMEM((1024, 512), BF),
            pltpu.SemaphoreType.DMA((14,)), pltpu.SemaphoreType.REGULAR, pltpu.SemaphoreType.REGULAR,
            pltpu.SemaphoreType.DMA((3,)), pltpu.SemaphoreType.DMA((3,)),
            pltpu.SemaphoreType.DMA((2,)), pltpu.SemaphoreType.DMA((2,)), sems, sems, sems, sems,
        ],
        compiler_params=pltpu.CompilerParams(
            collective_id=0, has_side_effects=True, vmem_limit_bytes=44 * 2**20),
        name="layer",
    )(*[pltpu.with_memory_space_constraint(a, pltpu.HBM) for a in (
        stream, outer_gate, inner_gate, conv_values, doc_ids.reshape(1, 256), conv_taps,
        norm_gain.reshape(1, 2048), route_ids.T, route_logits.T, group_weight.reshape(1, 128),
        out_weight, w_gate, w_up, w_down)])


def solution(mesh):
    placed = (
        P(("sp", "tp"), None),
        P("sp", "tp"),
        P("sp", "tp"),
        P("sp", "tp"),
        P("sp"),
        P(None, "tp"),
        P(),
        P(),
        P(("sp", "tp"), None),
        P(("sp", "tp"), None),
        P(("sp", "tp")),
        P(("sp", "tp"), None, None),
        P(("sp", "tp"), None, None),
        P(("sp", "tp"), None, None),
    )
    return jax.shard_map(
        on_device, mesh=mesh, in_specs=placed, out_specs=P(("sp", "tp"), None), check_vma=False
    )
```

```python
import functools

import jax
import jax.numpy as jnp
from jax import lax
from jax.experimental import pallas as pl
from jax.experimental.pallas import tpu as pltpu
from jax.sharding import PartitionSpec as P

MESH = pl.DeviceIdType.MESH
STEP = 59
BACK = pow(STEP, -1, 128)
SIZES = (32, 32, 32, 32)
CHUNKS = len(SIZES)
STARTS = [sum(SIZES[:c]) for c in range(CHUNKS)]
F32 = jnp.float32
BF = jnp.bfloat16


def partner(k, sign, sp, tp):
    o = lax.rem(k * STEP, 128)
    dz, dy, dx, dc = o // 32, lax.rem(o // 8, 4), lax.rem(o // 2, 4), lax.rem(o, 2)
    z, y, x = sp // 16, lax.rem(sp // 4, 4), lax.rem(sp, 4)
    if sign < 0:
        dz, dy, dx = 4 - dz, 4 - dy, 4 - dx
    there = lax.rem(z + dz, 4) * 16 + lax.rem(y + dy, 4) * 4 + lax.rem(x + dx, 4)
    return there, lax.rem(tp + dc, 2)


def dot(a, b):
    return jnp.dot(a, b, preferred_element_type=F32)


def iota(shape, dim):
    return lax.broadcasted_iota(jnp.int32, shape, dim)


def to_row(col, eye):
    return jnp.sum(jnp.where(eye, col, 0.0), axis=0, keepdims=True)


def to_col(row, eye):
    return jnp.sum(jnp.where(eye, row, 0.0), axis=1, keepdims=True)


def kernel(
    stream_hbm, outer_hbm, inner_hbm, values_hbm, docs_hbm, taps_hbm, gain_hbm, ids_hbm, logits_hbm, gw_hbm,
    ow_hbm, wg_hbm, wu_hbm, wd_hbm,
    out_ref,
    inner_ref, values_ref, docs_ref, outer_ref, taps_ref, ids_ref, logits_ref, gw_ref, stream_ref, gain_ref,
    ow, wg, wu, wd, product, mixed, edge, twin_edge, my_edge, docs_near, theirs, resid,
    nq, fold, unfold, outbox, inbox, outbox2, inbox2, xbuf, hbuf, yq, acc, masks,
    wsem, row_sem, plane_sem, esend, erecv, tsend, trecv, send1, recv1, send2, recv2,
):
    sp, tp = lax.axis_index("sp"), lax.axis_index("tp")
    pairs = [
        (inner_hbm, inner_ref), (values_hbm, values_ref), (docs_hbm, docs_ref), (outer_hbm, outer_ref),
        (taps_hbm, taps_ref), (ids_hbm, ids_ref), (logits_hbm, logits_ref), (gw_hbm, gw_ref),
        (stream_hbm, stream_ref), (gain_hbm, gain_ref), (ow_hbm, ow),
        (wg_hbm.at[0], wg), (wu_hbm.at[0], wu), (wd_hbm.at[0], wd),
    ]
    loads = [pltpu.make_async_copy(a, b, wsem.at[i]) for i, (a, b) in enumerate(pairs)]
    for load in loads[:11]:
        load.start()
    z, y, x = sp // 16, lax.rem(sp // 4, 4), lax.rem(sp, 4)

    def spot(dz, dy, dx):
        return lax.rem(z + dz, 4) * 16 + lax.rem(y + dy, 4) * 4 + lax.rem(x + dx, 4)

    def signal(sem, there, core):
        pl.semaphore_signal(sem, inc=1, device_id=(there, core), device_id_type=MESH)

    barrier = pltpu.get_barrier_semaphore()
    up, down = lax.rem(sp + 1, 64), lax.rem(sp + 63, 64)
    beside = jnp.where(tp == 0, down, up)
    for core in range(2):
        signal(barrier, beside, core)
    signal(barrier, sp, 1 - tp)
    for d in range(1, 4):
        for core in range(2):
            signal(barrier, spot(0, 0, d), core)
        signal(barrier, spot(0, d, 0), tp)
        signal(barrier, spot(d, 0, 0), tp)

    for load in loads[:3]:
        load.wait()
    product[...] = (inner_ref[...].astype(F32) * values_ref[...].astype(F32)).astype(BF)
    pl.semaphore_wait(barrier, 15)
    for d in range(1, 4):
        signal(row_sem, spot(0, d, 0), tp)

    def to_edge(source, target, n, m, there, core):
        return pltpu.make_async_remote_copy(
            src_ref=source, dst_ref=target, send_sem=esend.at[n], recv_sem=erecv.at[m],
            device_id=(there, core), device_id_type=MESH)

    edges = [
        to_edge(product.at[240:256], edge.at[tp], 0, tp, up, 0),
        to_edge(product.at[0:16], edge.at[tp], 1, tp, down, 1),
        to_edge(docs_ref, docs_near, 2, 2, jnp.where(tp == 0, up, down), tp),
    ]
    for copy in edges:
        copy.start()

    for load in loads[3:5]:
        load.wait()
    r0, r1 = iota((256, 256), 0), iota((256, 256), 1)
    docs = docs_ref[...].astype(F32)
    doc = to_col(docs, r0 == r1)
    same_prev = (to_col(docs, r0 == r1 + 1) == doc).astype(F32)
    same_next = (to_col(docs, r0 + 1 == r1) == doc).astype(F32)
    own = product[...].astype(F32)
    outer = outer_ref[...].astype(F32)
    tap = [taps_ref[k:k + 1, :] for k in range(3)]
    conv = tap[0] * pltpu.roll(own, 1, 0) * same_prev + tap[1] * own + tap[2] * pltpu.roll(own, 255, 0) * same_next
    mixed[...] = (outer * conv).astype(BF)
    base = [
        outer[0:1] * (tap[1] * own[0:1] + tap[2] * own[1:2] * same_next[0:1]),
        outer[255:256] * (tap[1] * own[255:256] + tap[0] * own[254:255] * same_prev[255:256]),
    ]
    coef = [outer[0:1] * tap[0], outer[255:256] * tap[2]]
    here = tp == 0
    my_base, my_coef = jnp.where(here, base[0], base[1]), jnp.where(here, coef[0], coef[1])
    my_edge[...] = jnp.where(
        iota((8, 512), 0) == 0, jnp.where(here, base[1], base[0]), jnp.where(here, coef[1], coef[0]))

    def to_twin(source, target, n):
        return pltpu.make_async_remote_copy(
            src_ref=source, dst_ref=target, send_sem=tsend.at[n], recv_sem=trecv.at[n],
            device_id=(sp, 1 - tp), device_id_type=MESH)

    twins = [
        to_twin(mixed.at[pl.ds(pl.multiple_of((1 - tp) * 128, 128), 128)], theirs, 0),
        to_twin(my_edge, twin_edge, 1),
    ]
    for copy in twins:
        copy.start()
    pl.semaphore_wait(row_sem, 3)
    for d in range(1, 4):
        signal(plane_sem, spot(d, 0, 0), tp)

    for load in loads[5:8]:
        load.wait()
    eye = iota((128, 128), 0) == iota((128, 128), 1)
    lane = iota((128, 128), 1)
    ids = [to_col(ids_ref[k:k + 1, :].astype(F32), eye).astype(jnp.int32) for k in range(2)]
    hot = [(ids[k] == lane).astype(F32) for k in range(2)]
    before = (iota((128, 128), 0) > lane).astype(BF)
    count = dot(before, (hot[0] + hot[1]).astype(BF))
    slots, slot_rows = [], []
    for k in range(2):
        e = ids[k]
        dz = ((e >> 5) + (4 - z)) & 3
        dy = (((e >> 3) & 3) + (4 - y)) & 3
        dx = (((e >> 1) & 3) + (4 - x)) & 3
        dc = ((e & 1) + (2 - tp)) & 1
        o = dz * 32 + dy * 8 + dx * 2 + dc
        place = (o * BACK) & 127
        rank = jnp.sum(hot[k] * count, axis=1, keepdims=True)
        slot = place.astype(F32) * 4.0 + rank
        slots.append(slot.astype(jnp.int32))
        slot_rows.append(to_row(slot, eye).astype(jnp.int32))
    expo = jnp.exp(logits_ref[...])
    total = expo[0:1, :] + expo[1:2, :]
    gates = [to_col(gw_ref[...] * expo[k:k + 1, :] / total, eye) for k in range(2)]

    def copy_out(k, c):
        rows = pl.ds(pl.multiple_of(k * 16, 16), 16)
        return pltpu.make_async_remote_copy(
            src_ref=outbox.at[rows], dst_ref=inbox.at[rows], send_sem=send1.at[c], recv_sem=recv1.at[c],
            device_id=partner(k, 1, sp, tp), device_id_type=MESH)

    def copy_back(k, c):
        rows = pl.ds(pl.multiple_of(k * 16, 16), 16)
        return pltpu.make_async_remote_copy(
            src_ref=outbox2.at[rows], dst_ref=inbox2.at[rows], send_sem=send2.at[c], recv_sem=recv2.at[c],
            device_id=partner(k, -1, sp, tp), device_id_type=MESH)

    def mask(c):
        base, size = STARTS[c] * 16, SIZES[c] * 16
        at = iota((size, 128), 0) + base
        mine = ((at >> 2) == slot_rows[0]) | ((at >> 2) == slot_rows[1])
        return jnp.concatenate([(mine & ((at & 3) == q)).astype(BF) for q in range(4)], axis=1)

    def pack(c, chosen):
        base, size = STARTS[c] * 16, SIZES[c] * 16
        outbox[base:base + size, :] = dot(chosen, nq[...]).astype(BF)

    def picks(c, q):
        at = iota((128, SIZES[c] * 16), 1) + STARTS[c] * 16
        return jnp.concatenate([(at == slots[k] * 4 + q).astype(BF) for k in range(2)], axis=0)

    def span(c):
        first = max(1, STARTS[c])
        return pl.ds(first * 16, (STARTS[c] + SIZES[c] - first) * 16)

    for copy in edges:
        copy.wait_send()
    for half in range(2):
        to_edge(product.at[0:16], edge.at[half], 0, half, up, 0).wait_recv()
    edges[2].wait_recv()
    for copy in twins:
        copy.wait()
    beyond = jnp.where(here, docs_near[:, 255:256], docs_near[:, 0:1])
    at_edge = jnp.where(here, docs_ref[:, 0:1], docs_ref[:, 255:256])
    inside = jnp.where(here, sp > 0, sp < 63)
    same = jnp.where((beyond == at_edge) & inside, 1.0, 0.0)

    def place_edge(box, start, half, base_row, coef_row):
        rows = pl.ds(pl.multiple_of(start + tp * 112, 16), 16)
        block = edge[half].astype(F32)
        near_row = jnp.where(here, block[15:16], block[0:1])
        value = base_row + coef_row * near_row * same
        box[rows, :] = jnp.where(iota((16, 512), 0) == tp * 15, value, box[rows, :].astype(F32)).astype(BF)

    place_edge(mixed, tp * 128, tp, my_base, my_coef)
    place_edge(theirs, 0, 1 - tp, twin_edge[0:1, :], twin_edge[1:2, :])

    for load in loads[8:11]:
        load.wait()
    for load in loads[11:]:
        load.start()
    mine = pl.ds(pl.multiple_of(tp * 128, 128), 128)
    near = pl.ds(pl.multiple_of(tp * 512, 512), 512)
    far = pl.ds(pl.multiple_of((1 - tp) * 512, 512), 512)
    square = jnp.zeros((128, 1), F32)
    for q in range(4):
        cols = slice(q * 512, (q + 1) * 512)
        value = stream_ref[:, cols].astype(F32) + (
            dot(mixed[mine, :], ow[near, cols]) + dot(theirs[...], ow[far, cols]))
        resid[:, cols] = value
        square += jnp.sum(value * value, axis=1, keepdims=True)
    scale = lax.rsqrt(square / 2048.0 + 1e-06)
    for q in range(4):
        cols = slice(q * 512, (q + 1) * 512)
        nq[q * 128:(q + 1) * 128, :] = (resid[:, cols] * scale * gain_ref[:, cols]).astype(BF)

    pack(0, mask(0))
    pl.semaphore_wait(plane_sem, 3)
    for c in range(CHUNKS):
        @pl.loop(max(1, STARTS[c]), STARTS[c] + SIZES[c])
        def _(k):
            copy_out(k, c).start()
        if c + 1 < CHUNKS:
            pack(c + 1, mask(c + 1))
    inbox[0:16, :] = outbox[0:16, :]
    m = iota((512, 512), 0)
    n = iota((512, 512), 1)
    fold[...] = (m == (n & 127) * 4 + (n >> 7)).astype(BF)
    unfold[...] = (n == (m & 127) * 4 + (m >> 7)).astype(BF)
    for load in loads[11:]:
        load.wait()

    for c in range(CHUNKS):
        s = span(c)
        pltpu.make_async_copy(inbox.at[s], inbox.at[s], recv1.at[c]).wait()
        box = slice(STARTS[c] * 16, (STARTS[c] + SIZES[c]) * 16)
        rows, size = SIZES[c] * 4, SIZES[c] * 16
        for q in range(4):
            xq = dot(unfold[q * 128:q * 128 + rows, :size], inbox[box, :])
            xbuf[:rows, q * 512:(q + 1) * 512] = xq.astype(BF)

        @pl.loop(0, 4)
        def _(n):
            cols = pl.ds(pl.multiple_of(n * 256, 256), 256)
            g = dot(xbuf[:rows, :], wg[:, cols])
            u = dot(xbuf[:rows, :], wu[:, cols])
            hbuf[:rows, cols] = (g / (1.0 + jnp.exp(-g)) * u).astype(BF)

        @pl.loop(0, 4)
        def _(q):
            cols = pl.ds(pl.multiple_of(q * 512, 512), 512)
            yq[pl.ds(pl.multiple_of(q * 128, 128), rows), :] = dot(hbuf[:rows, :], wd[:, cols]).astype(BF)

        outbox2[box, :] = dot(fold[:size, :], yq[...]).astype(BF)

        @pl.loop(max(1, STARTS[c]), STARTS[c] + SIZES[c])
        def _(k):
            copy_back(k, c).start()
    inbox2[0:16, :] = outbox2[0:16, :]

    for c in range(CHUNKS):
        s = span(c)
        final = c + 1 == CHUNKS
        if final:
            for q in range(4):
                masks[q * 256:(q + 1) * 256, :] = picks(c, q)
        pltpu.make_async_copy(inbox2.at[s], inbox2.at[s], recv2.at[c]).wait()
        box = slice(STARTS[c] * 16, (STARTS[c] + SIZES[c]) * 16)
        for q in range(4):
            cols = slice(q * 512, (q + 1) * 512)
            pick = masks[q * 256:(q + 1) * 256, :] if final else picks(c, q)
            found = dot(pick, inbox2[box, :])
            if c == 0:
                acc[:, cols] = found
            elif c + 1 < CHUNKS:
                acc[:, cols] += found
            else:
                found = found + acc[:, cols]
                out_ref[:, cols] = (
                    resid[:, cols] + (gates[0] * found[:128] + gates[1] * found[128:])).astype(BF)
    for c in range(CHUNKS):
        s = span(c)
        pltpu.make_async_copy(outbox.at[s], outbox.at[s], send1.at[c]).wait()
        pltpu.make_async_copy(outbox2.at[s], outbox2.at[s], send2.at[c]).wait()


def on_device(
    stream, outer_gate, inner_gate, conv_values, doc_ids, conv_taps, out_weight, norm_gain,
    route_ids, route_logits, group_weight, w_gate, w_up, w_down,
):
    vmem = pl.BlockSpec(memory_space=pltpu.VMEM)
    hbm = pl.BlockSpec(memory_space=pltpu.HBM)
    box = pltpu.VMEM((2048, 512), BF)
    sems = pltpu.SemaphoreType.DMA((CHUNKS,))
    docs = pltpu.VMEM((1, 256), jnp.int32)
    edge = pltpu.VMEM((8, 512), F32)
    return pl.pallas_call(
        kernel,
        out_shape=jax.ShapeDtypeStruct((128, 2048), BF),
        in_specs=[hbm] * 14,
        out_specs=vmem,
        scratch_shapes=[
            pltpu.VMEM((256, 512), BF), pltpu.VMEM((256, 512), BF), docs, pltpu.VMEM((256, 512), BF),
            pltpu.VMEM((3, 512), F32), pltpu.VMEM((2, 128), jnp.int32), pltpu.VMEM((2, 128), F32),
            pltpu.VMEM((1, 128), F32), pltpu.VMEM((128, 2048), BF), pltpu.VMEM((1, 2048), F32),
            pltpu.VMEM((1024, 2048), BF),
            pltpu.VMEM((2048, 1024), BF), pltpu.VMEM((2048, 1024), BF), pltpu.VMEM((1024, 2048), BF),
            pltpu.VMEM((256, 512), BF), pltpu.VMEM((256, 512), BF), pltpu.VMEM((2, 16, 512), BF), edge, edge, docs,
            pltpu.VMEM((128, 512), BF), pltpu.VMEM((128, 2048), F32),
            pltpu.VMEM((512, 512), BF), pltpu.VMEM((512, 512), BF), pltpu.VMEM((512, 512), BF),
            box, box, box, box,
            pltpu.VMEM((128, 2048), BF), pltpu.VMEM((128, 1024), BF), pltpu.VMEM((512, 512), BF),
            pltpu.VMEM((256, 2048), F32), pltpu.VMEM((1024, 512), BF),
            pltpu.SemaphoreType.DMA((14,)), pltpu.SemaphoreType.REGULAR, pltpu.SemaphoreType.REGULAR,
            pltpu.SemaphoreType.DMA((3,)), pltpu.SemaphoreType.DMA((3,)),
            pltpu.SemaphoreType.DMA((2,)), pltpu.SemaphoreType.DMA((2,)), sems, sems, sems, sems,
        ],
        compiler_params=pltpu.CompilerParams(
            collective_id=0, has_side_effects=True, vmem_limit_bytes=44 * 2**20),
        name="layer",
    )(*[pltpu.with_memory_space_constraint(a, pltpu.HBM) for a in (
        stream, outer_gate, inner_gate, conv_values, doc_ids.reshape(1, 256), conv_taps,
        norm_gain.reshape(1, 2048), route_ids.T, route_logits.T, group_weight.reshape(1, 128),
        out_weight, w_gate, w_up, w_down)])


def solution(mesh):
    placed = (
        P(("sp", "tp"), None),
        P("sp", "tp"),
        P("sp", "tp"),
        P("sp", "tp"),
        P("sp"),
        P(None, "tp"),
        P(),
        P(),
        P(("sp", "tp"), None),
        P(("sp", "tp"), None),
        P(("sp", "tp")),
        P(("sp", "tp"), None, None),
        P(("sp", "tp"), None, None),
        P(("sp", "tp"), None, None),
    )
    return jax.shard_map(
        on_device, mesh=mesh, in_specs=placed, out_specs=P(("sp", "tp"), None), check_vma=False
    )
```
